32 devices in a mesh: sp: 8 (over z, y), tp: 4 (over x, core).
Axes of the slice: x: 2, y: 2, z: 4, core: 2. Of those that a mesh axis runs over, the one named last changes fastest.
Arguments:
- queries: bfloat16 [2048, 1024], P('sp', 'tp'), may hold values from -8 to 8
- keys: bfloat16 [2048, 256], P('sp', 'tp'), may hold values from -6 to 6
- values: bfloat16 [2048, 256], P('sp', 'tp'), may hold values from -6 to 6
- query_gain: float32 [64], replicated, may hold values from 0.3 to 9
- key_norm_gain: float32 [64], replicated, may hold values from 0.3 to 9
- attn_gain: float32 [1024], replicated, may hold values from 0.1 to 1.9
- residual: bfloat16 [2048, 2048], P('sp', 'tp'), may hold values from -20 to 20
- out_weight: bfloat16 [1024, 2048], P(None, 'tp'), may hold values from -0.1875 to 0.1875
- ffn_gain: float32 [2048], P('tp'), may hold values from 0.1 to 1.9
- routes: int32 [2048, 4], P('sp'), may hold values from 0 to 7, all different within a row; in each aligned block of 256 rows (0 to 255, 256 to 511, ...) at most 192 rows name the same one
- route_weight: float32 [2048, 4], P('sp'), may hold values from 0.2 to 1
- gate_weight: bfloat16 [8, 2048, 2048], P('sp', None, 'tp'), may hold values from -0.5 to 0.5
- up_weight: bfloat16 [8, 2048, 2048], P('sp', None, 'tp'), may hold values from -0.5 to 0.5
- down_weight: bfloat16 [8, 2048, 2048], P('sp', 'tp'), may hold values from -0.0068359375 to 0.0068359375
Outputs:
- layer_out: bfloat16 [2048, 2048], P('sp', 'tp')
The draws below stay inside these ranges and needn't reach their ends.
Inputs may be any that keep to these rules, and one draw needn't show every extreme that they name: Each token names 4 different experts. In the tokens of one index of sp (aligned blocks of 256 tokens) no expert is named by more than 192 routes, a bound that some block reaches.
All inputs are finite; a program needn't handle non-finite values.
Results may differ from the reference program's by a relative error of at most 0.012.
The reference program's roundings to bfloat16 on the way count: a program that leaves them out, or rounds other values in their place, can miss the bound.
Values may be sent and summed in bfloat16 or wider, within the bound.
A program may use at most 64 MiB of HBM per device.

```python
import math
import jax
import jax.numpy as jnp
import numpy as np
from jax import lax

D = 2048
FF = 2048
HEAD_DIMENSION = 64
QUERY_HEADS = 16
KEY_VALUE_HEADS = 4
TOPK = 4
GRID_W = 64
TOK_SP = 256
SEQUENCE_TOKENS = 2048
EXPERTS = 8
CAP = 192
N_SP = 8
N_TP = 4


def gain_values(key, salt_value):
    noise_sample = jax.random.uniform(jax.random.fold_in(key, salt_value), (HEAD_DIMENSION,), jnp.float32)
    return 0.5 + noise_sample


def draw_query_gain(key, part):
    return gain_values(key, 502)


def draw_key_norm_gain(key, part):
    return gain_values(key, 503)


def key_head_rows(key):
    baseline_sample = jax.random.normal(jax.random.fold_in(key, 601), (SEQUENCE_TOKENS, KEY_VALUE_HEADS, HEAD_DIMENSION), jnp.float32)
    return jnp.clip(baseline_sample, -6.0, 6.0)


def draw_keys(key, part):
    return key_head_rows(key).reshape(SEQUENCE_TOKENS, KEY_VALUE_HEADS * HEAD_DIMENSION).astype(jnp.bfloat16)


def draw_queries(key, part):
    group_width = QUERY_HEADS // KEY_VALUE_HEADS
    noise_sample = jax.random.normal(jax.random.fold_in(key, 602), (SEQUENCE_TOKENS, KEY_VALUE_HEADS, group_width, HEAD_DIMENSION), jnp.float32)
    return jnp.clip(noise_sample, -8.0, 8.0).reshape(SEQUENCE_TOKENS, QUERY_HEADS * HEAD_DIMENSION).astype(jnp.bfloat16)


def draw_residual(key, part):
    columns = jnp.arange(D, dtype=jnp.float32) / D
    baseline_sample = jnp.clip(jax.random.normal(jax.random.fold_in(key, 701), (SEQUENCE_TOKENS, D), jnp.float32), -6.0, 6.0)
    column_scale = 0.6 * jnp.exp(jnp.log(5.0) * columns)
    return (baseline_sample * column_scale[None, :]).astype(jnp.bfloat16)


def level_of(own_key, shape, cuts, low, high):
    def one(position, blocks):
        steps = jax.random.uniform(jax.random.fold_in(jax.random.fold_in(own_key, 6), position), (blocks,), jnp.float32, low / len(cuts), high / len(cuts))
        return jnp.repeat(jnp.exp(steps), shape[position] // blocks).reshape((-1,) + (1,) * (len(shape) - position - 1))

    loudness = one(*cuts[0])
    for cut in cuts[1:]:
        loudness = loudness * one(*cut)
    return loudness


def deal_out(rng, own, number, rows, number_of, top, limit, slope):
    ranking = jax.random.permutation(rng, number_of)
    packed, usual = load_shares(number_of, rows * top, limit, slope, True), load_shares(number_of, rows * top, limit, slope, False)
    places = jnp.arange(number_of)

    def named(sizes, offset_by):
        used = int((sizes > 0).sum())
        fixed = max(1, used // 4)
        shifted = fixed + (places - fixed + offset_by * (used - fixed)) % max(1, number_of - fixed)
        return jnp.zeros((number_of,), jnp.int32).at[ranking[jnp.where(places < fixed, places, shifted)]].set(jnp.asarray(sizes, jnp.int32))

    sizes = jnp.where(number % 4 == 0, named(packed, number // 4), named(usual, number - number // 4 - 1))
    mixed = jax.random.permutation(jax.random.fold_in(own, 3), number_of)
    donor, taker = mixed[0:number_of // 2 * 2:2], mixed[1:number_of // 2 * 2:2]
    room = jnp.minimum(sizes[donor] - 1, limit - sizes[taker]) // 2
    room = jnp.where((donor == ranking[0]) | (taker == ranking[0]) | (sizes[taker] == 0), 0, jnp.maximum(room, 0))
    shifted = jax.random.randint(jax.random.fold_in(own, 4), (number_of // 2,), 0, 1 << 20) % (room + 1)
    sizes = sizes.at[donor].add(-shifted).at[taker].add(shifted)
    labels = jnp.searchsorted(jnp.cumsum(sizes), jnp.arange(rows * top), side="right").astype(jnp.int32)
    listing = labels.reshape(top, rows).T
    listing = listing[jax.random.permutation(jax.random.fold_in(own, 1), rows)]
    offset_by = jax.random.randint(jax.random.fold_in(own, 2), (rows, 1), 0, top)
    return jnp.take_along_axis(listing, (jnp.arange(top)[None, :] + offset_by) % top, axis=1)


def load_shares(amount, total, most, lean, full):
    weights = [(1 << 20) // math.isqrt(grade ** lean) + 1 for grade in range(1, amount + 1)]
    largest = most if full else min(most, max(-(-total // amount), total * weights[0] // sum(weights)))
    least = 1 if total - largest >= amount - 1 else 0
    given, spare = [largest] + [least] * (amount - 1), total - largest - least * (amount - 1)
    while spare > 0:
        free = [i for i in range(1, amount) if given[i] < largest] or [i for i in range(1, amount) if given[i] < most]
        pool, left = sum([weights[i] for i in free]), spare
        for i in free:
            addition = min(most - given[i], max(1, left * weights[i] // pool), spare)
            given[i] = given[i] + addition
            spare = spare - addition
    return np.array(given)


def normal_values(key, shape, deviation, most, cuts=(), held_as=jnp.bfloat16):
    loudness = level_of(key, shape, cuts, -0.22, 0.18) if cuts else 1.0
    drawn = jax.random.normal(key, shape, jnp.float32) * deviation * loudness
    return jnp.minimum(jnp.maximum(drawn, -most), most).astype(held_as)


def setup_inputs(seed: int = 0) -> dict:
    key_of = jax.random.split(jax.random.key(seed), 15)
    queries = draw_queries(jax.random.fold_in(key_of[14], 71), 0)
    keys = draw_keys(jax.random.fold_in(key_of[14], 71), 0)
    values = normal_values(key_of[2], (SEQUENCE_TOKENS, KEY_VALUE_HEADS * HEAD_DIMENSION), 1.0, 6.0, ((0, 8), (1, 4)))
    query_gain = draw_query_gain(jax.random.fold_in(key_of[14], 71), 0)
    key_norm_gain = draw_key_norm_gain(jax.random.fold_in(key_of[14], 71), 0)
    attn_gain = jnp.clip(1.0 + 0.18 * jax.random.normal(key_of[5], (QUERY_HEADS * HEAD_DIMENSION,), jnp.float32), 0.1, 1.9)
    residual = draw_residual(jax.random.fold_in(key_of[14], 71), 0)
    out_weight = normal_values(key_of[7], (QUERY_HEADS * HEAD_DIMENSION, D), (QUERY_HEADS * HEAD_DIMENSION) ** -0.5, 0.1875, ((1, 4),))
    ffn_gain = jnp.clip(1.0 + 0.18 * jax.random.normal(key_of[8], (D,), jnp.float32), 0.1, 1.9)
    routes_keys = jax.random.split(jax.random.fold_in(key_of[9], 1), SEQUENCE_TOKENS // TOK_SP)
    routes_turns = jax.random.permutation(jax.random.fold_in(key_of[9], 3), SEQUENCE_TOKENS // TOK_SP)
    routes = jax.vmap(lambda own, number: deal_out(jax.random.fold_in(key_of[9], 2), own, number, TOK_SP, EXPERTS, TOPK, CAP, 2))(routes_keys, routes_turns).reshape((SEQUENCE_TOKENS, TOPK))
    route_weight = jnp.clip(0.2 + 0.8 * jax.random.uniform(key_of[10], (SEQUENCE_TOKENS, TOPK), jnp.float32) ** level_of(key_of[10], (SEQUENCE_TOKENS, TOPK), ((0, 8),), -0.2, 0.2), 0.2, 1.0)
    gate_weight = normal_values(key_of[11], (EXPERTS, D, FF), (D // 16) ** -0.5, 0.5, ((0, 8), (2, 4)))
    up_weight = normal_values(key_of[12], (EXPERTS, D, FF), (D // 16) ** -0.5, 0.5, ((0, 8), (2, 4)))
    down_weight = normal_values(key_of[13], (EXPERTS, FF, D), (FF * 400) ** -0.5, 0.0068359375, ((0, 8), (1, 4)))
    return dict(queries=queries, keys=keys, values=values, query_gain=query_gain, key_norm_gain=key_norm_gain, attn_gain=attn_gain, residual=residual, out_weight=out_weight, ffn_gain=ffn_gain, routes=routes, route_weight=route_weight, gate_weight=gate_weight, up_weight=up_weight, down_weight=down_weight)


EPS = 1e-06
THETA = 10000.0
ALPHA = 1.702
LIMIT = 7.0

def rotary_tables(positions, head_size, grid_width):
    row_pos = (positions // grid_width).astype(jnp.float32)
    col_pos = (positions % grid_width).astype(jnp.float32)
    half_size = head_size // 2
    inverse = THETA ** (-jnp.arange(0, half_size, 2, dtype=jnp.float32) / half_size)
    angles = jnp.concatenate([row_pos[:, None] * inverse, col_pos[:, None] * inverse], axis=-1)
    return (jnp.cos(angles), jnp.sin(angles))

def normalize_then_rotate(head_rows, gain_vector, cosine_lookup, sine_lookup):
    values_f = head_rows.astype(jnp.float32)
    scaled = values_f * lax.rsqrt(lax.optimization_barrier(jnp.mean(values_f * values_f, axis=-1, keepdims=True)) + EPS) * gain_vector
    first_half, second_half = jnp.split(scaled, 2, axis=-1)
    cos_part = cosine_lookup[:, None, :]
    sin_part = sine_lookup[:, None, :]
    return jnp.concatenate([first_half * cos_part - second_half * sin_part, first_half * sin_part + second_half * cos_part], axis=-1).astype(jnp.bfloat16)

def clamped_unit(gate_sum, up_sum):
    gate_sum = jnp.minimum(gate_sum, LIMIT)
    up_sum = jnp.clip(up_sum, -LIMIT, LIMIT)
    return ((up_sum + 1.0) * gate_sum * jax.nn.sigmoid(ALPHA * gate_sum)).astype(jnp.bfloat16)

def reference(queries, keys, values, query_gain, key_norm_gain, attn_gain, residual, out_weight, ffn_gain, routes, route_weight, gate_weight, up_weight, down_weight):
    group_width = QUERY_HEADS // KEY_VALUE_HEADS
    positions = jnp.arange(SEQUENCE_TOKENS, dtype=jnp.int32)
    cosine_lookup, sine_lookup = rotary_tables(positions, HEAD_DIMENSION, GRID_W)
    query_rotated = normalize_then_rotate(queries.reshape(SEQUENCE_TOKENS, QUERY_HEADS, HEAD_DIMENSION), query_gain, cosine_lookup, sine_lookup)
    query_rotated = query_rotated.reshape(SEQUENCE_TOKENS // 256, 256, KEY_VALUE_HEADS, group_width, HEAD_DIMENSION)
    key_rotated = normalize_then_rotate(keys.reshape(SEQUENCE_TOKENS, KEY_VALUE_HEADS, HEAD_DIMENSION), key_norm_gain, cosine_lookup, sine_lookup).astype(jnp.float32)
    value_float = values.reshape(SEQUENCE_TOKENS, KEY_VALUE_HEADS, HEAD_DIMENSION).astype(jnp.float32)

    def attend(query_block):
        query_f = query_block.astype(jnp.float32)
        scores = jnp.einsum('qkgd,nkd->kgqn', query_f, key_rotated) * HEAD_DIMENSION ** (-0.5)
        row_max = lax.optimization_barrier(jnp.max(scores, axis=-1, keepdims=True))
        weights = jnp.exp(scores - row_max)
        row_sum = lax.optimization_barrier(jnp.sum(weights, axis=-1))
        mixed = jnp.einsum('kgqn,nkd->qkgd', weights.astype(jnp.bfloat16).astype(jnp.float32), value_float)
        return mixed / jnp.transpose(row_sum, (2, 0, 1))[..., None]
    attended = lax.map(attend, query_rotated).reshape(SEQUENCE_TOKENS, QUERY_HEADS * HEAD_DIMENSION).astype(jnp.bfloat16)
    head_f = attended.astype(jnp.float32)
    attn_normed = (head_f * lax.rsqrt(lax.optimization_barrier(jnp.mean(head_f * head_f, axis=-1, keepdims=True)) + EPS) * attn_gain).astype(jnp.bfloat16)
    mid_stream = (residual.astype(jnp.float32) + jnp.dot(attn_normed, out_weight, preferred_element_type=jnp.float32)).astype(jnp.bfloat16)
    mid_f = mid_stream.astype(jnp.float32)
    ffn_in = (mid_f * lax.rsqrt(lax.optimization_barrier(jnp.mean(mid_f * mid_f, axis=-1, keepdims=True)) + EPS) * ffn_gain).astype(jnp.bfloat16)
    blocks = N_SP
    route_list = routes.reshape(blocks, TOK_SP * TOPK)
    onehot = (route_list[..., None] == jnp.arange(EXPERTS, dtype=jnp.int32)[None, None, :]).astype(jnp.int32)
    route_ranks = lax.optimization_barrier(jnp.sum((jnp.cumsum(onehot, axis=1) - 1) * onehot, axis=2))
    block_ids = jnp.arange(blocks, dtype=jnp.int32)[:, None]
    slot_index = (route_list * (blocks * CAP) + block_ids * CAP + route_ranks).reshape(-1)
    token_ids = (block_ids * TOK_SP + jnp.arange(TOK_SP * TOPK, dtype=jnp.int32)[None, :] // TOPK).reshape(-1)
    slot_owner = jnp.full((EXPERTS * blocks * CAP,), SEQUENCE_TOKENS, jnp.int32).at[slot_index].set(token_ids)
    padded = jnp.concatenate([ffn_in, jnp.zeros((1, D), jnp.bfloat16)], axis=0)
    dispatched = padded[slot_owner].reshape(EXPERTS, blocks * CAP, D)

    def expert(operands):
        slot_rows, w_gate, w_up, w_down = operands
        gate_sum = jnp.dot(slot_rows, w_gate, preferred_element_type=jnp.float32)
        up_sum = jnp.dot(slot_rows, w_up, preferred_element_type=jnp.float32)
        activation = clamped_unit(gate_sum, up_sum)
        parts = jnp.einsum('rjf,jfd->jrd', activation.reshape(-1, N_TP, FF // N_TP).astype(jnp.float32), w_down.reshape(N_TP, FF // N_TP, D).astype(jnp.float32))
        return lax.optimization_barrier(jnp.sum(parts.astype(jnp.bfloat16).astype(jnp.float32), axis=0)).astype(jnp.bfloat16)
    expert_out = lax.map(expert, (dispatched, gate_weight, up_weight, down_weight))
    picked = expert_out.reshape(-1, D)[slot_index].astype(jnp.float32)
    weighted = lax.optimization_barrier(jnp.sum((picked * route_weight.reshape(-1)[:, None]).reshape(SEQUENCE_TOKENS, TOPK, D), axis=1))
    return (mid_f + weighted).astype(jnp.bfloat16)
```

```python
import functools

import jax
import jax.numpy as jnp
import numpy as np
from jax import lax
from jax.experimental import pallas as pl
from jax.experimental.pallas import tpu as pltpu
from jax.sharding import PartitionSpec as P

D = 2048
GRID_W = 64


EPS = 1e-06
THETA = 10000.0
ALPHA = 1.702
LIMIT = 7.0


def rotary_tables(positions, head_size, grid_width):
    row_pos = (positions // grid_width).astype(jnp.float32)
    col_pos = (positions % grid_width).astype(jnp.float32)
    half_size = head_size // 2
    inverse = THETA ** (-jnp.arange(0, half_size, 2, dtype=jnp.float32) / half_size)
    angles = jnp.concatenate([row_pos[:, None] * inverse, col_pos[:, None] * inverse], axis=-1)
    return (jnp.cos(angles), jnp.sin(angles))


def normalize_then_rotate(head_rows, gain_vector, cosine_lookup, sine_lookup):
    values_f = head_rows.astype(jnp.float32)
    scaled = (
        values_f
        * lax.rsqrt(jnp.mean(values_f * values_f, axis=-1, keepdims=True) + EPS)
        * gain_vector
    )
    first_half, second_half = jnp.split(scaled, 2, axis=-1)
    cos_part = cosine_lookup[:, None, :]
    sin_part = sine_lookup[:, None, :]
    return jnp.concatenate(
        [
            first_half * cos_part - second_half * sin_part,
            first_half * sin_part + second_half * cos_part,
        ],
        axis=-1,
    ).astype(jnp.bfloat16)


def clamped_unit(gate_sum, up_sum):
    gate_sum = jnp.minimum(gate_sum, LIMIT)
    up_sum = jnp.clip(up_sum, -LIMIT, LIMIT)
    return ((up_sum + 1.0) * gate_sum * jax.nn.sigmoid(ALPHA * gate_sum)).astype(jnp.bfloat16)


def ring_place(device, n):
    odd = lax.rem(device, 2)
    far = device // 2
    return (1 - odd) * far + odd * (n - 1 - far)


def ring_device(place, n):
    odd = place // (n // 2)
    return 2 * ((1 - odd) * place + odd * (n - 1 - place)) + odd


def expert_kernel(
    n, x_ref, share_ref, gate_hbm, up_hbm, down_hbm, out_ref,
    gate_ref, up_ref, down_ref, held, core_out, core_in, ring_in, ring_out, kept, first, last_out, last_in,
    w_sem, local_sem, x_send, x_recv, g_send, g_recv, c_send, c_recv,
    cs_send, cs_recv, r_send, r_recv, l_send, l_recv,
):
    me = lax.axis_index("sp")
    tp = lax.axis_index("tp")
    core = lax.rem(tp, 2)
    side = tp // 2
    place = ring_place(me, n)
    after = ring_device(lax.rem(place + 1, n), n)
    before = ring_device(lax.rem(place + n - 1, n), n)
    targets = (after, before)
    other_core = side * 2 + 1 - core
    other_side = (1 - side) * 2 + core
    half = held.shape[4]
    width = held.shape[5]

    loads = [
        pltpu.make_async_copy(src.at[0], dst, w_sem.at[i])
        for i, (src, dst) in enumerate(((gate_hbm, gate_ref), (up_hbm, up_ref), (down_hbm, down_ref)))
    ]
    for load in loads:
        load.start()

    barrier = pltpu.get_barrier_semaphore()
    for peer in ((after, tp), (before, tp), (me, other_core), (me, other_side)):
        pl.semaphore_signal(barrier, inc=1, device_id=peer, device_id_type=pl.DeviceIdType.MESH)
    pl.semaphore_wait(barrier, 4)

    def remote(src, dst, send, recv, peer):
        return pltpu.make_async_remote_copy(
            src_ref=src, dst_ref=dst, send_sem=send, recv_sem=recv,
            device_id=peer, device_id_type=pl.DeviceIdType.MESH,
        )

    def owner(h, step):
        return ring_device(lax.rem(place + (n - step if h == 0 else step), n), n)

    def side_copy(h):
        return remote(
            x_ref.at[pl.ds(h * half, half)], held.at[me, h, core, side],
            x_send.at[h], x_recv.at[h], (me, other_side),
        )

    def side_arrival(h):
        return remote(
            x_ref.at[pl.ds(h * half, half)], held.at[me, h, core, 1 - side],
            x_send.at[h], x_recv.at[h], (me, other_side),
        )

    def ring_copy(h, step):
        block = held.at[owner(h, step), h, core]
        return remote(block, block, g_send.at[h, step], g_recv.at[h, step + 1], (targets[h], tp))

    def ring_arrival(h, step):
        block = held.at[owner(h, step), h, core]
        return remote(block, block, g_send.at[h, step], g_recv.at[h, step], (targets[h], tp))

    def core_copy(h, step):
        block = held.at[owner(h, step), h, core]
        return remote(block, block, c_send.at[h, step], c_recv.at[h, step], (me, other_core))

    def core_arrival(h, step):
        block = held.at[owner(h, step), h, 1 - core]
        return remote(block, block, c_send.at[h, step], c_recv.at[h, step], (me, other_core))

    def sums_copy(step):
        return remote(
            core_out.at[step], core_in.at[step], cs_send.at[step], cs_recv.at[step], (me, other_core)
        )

    def total_copy(h, step):
        later = lax.rem(step + 1, n)
        return remote(
            ring_out.at[step, h], ring_in.at[later, h],
            r_send.at[h, step], r_recv.at[h, later], (targets[h], tp),
        )

    def total_arrival(h, step):
        return remote(
            ring_out.at[step, h], ring_in.at[step, h],
            r_send.at[h, step], r_recv.at[h, step], (targets[h], tp),
        )

    locals_ = [
        pltpu.make_async_copy(
            x_ref.at[pl.ds(h * half, half)], held.at[me, h, core, side], local_sem.at[h]
        )
        for h in range(2)
    ]
    for h in range(2):
        side_copy(h).start()
        locals_[h].start()
    ring_in[1] = jnp.zeros(ring_in.shape[1:], ring_in.dtype)
    for h in range(2):
        locals_[h].wait()
        side_arrival(h).wait_recv()

    def one_step(step, carry):
        @pl.when(step > 0)
        def _():
            for h in range(2):
                ring_arrival(h, step).wait_recv()

        @pl.when(step < n - 1)
        def _():
            for h in range(2):
                ring_copy(h, step).start()

        for h in range(2):
            core_copy(h, step).start()

        @pl.when(step == 0)
        def _():
            for load in loads:
                load.wait()

        for h in range(2):
            core_arrival(h, step).wait_recv()
        owners = (owner(0, step), owner(1, step))
        rows = jnp.concatenate(
            [
                jnp.concatenate([held[owners[h], h, t % 2, t // 2] for t in range(4)], axis=1)
                for h in range(2)
            ],
            axis=0,
        )
        gate_sum = jnp.dot(rows, gate_ref[...], preferred_element_type=jnp.float32)
        up_sum = jnp.dot(rows, up_ref[...], preferred_element_type=jnp.float32)
        units = clamped_unit(gate_sum, up_sum)
        share = jnp.concatenate([share_ref[owners[h], h] for h in range(2)], axis=0)
        share = jnp.concatenate([share] * (width // 128), axis=1)

        def part_of(which, x):
            columns = pl.ds(pl.multiple_of((2 * x + which) * width, width), width)
            return jnp.dot(units, down_ref[:, columns], preferred_element_type=jnp.float32) * share

        for x in range(2):
            part = part_of(1 - core, x).astype(jnp.bfloat16)
            for h in range(2):
                core_out[step, h, x] = part[h * half : (h + 1) * half]
        sums_copy(step).start()
        for x in range(2):
            part = part_of(core, x)
            for h in range(2):
                kept[h, x] = part[h * half : (h + 1) * half]
        sums_copy(step).wait_recv()

        @pl.when(step == 0)
        def _():
            first[...] = kept[...] + core_in[0].astype(jnp.float32)

        @pl.when(step > 0)
        def _():
            for h in range(2):
                @pl.when(step > 1)
                def _():
                    total_arrival(h, step).wait_recv()

                total = kept[h] + core_in[step, h].astype(jnp.float32)
                ring_out[step, h] = (total + ring_in[step, h].astype(jnp.float32)).astype(jnp.bfloat16)
                total_copy(h, step).start()

        return carry

    lax.fori_loop(0, n, one_step, 0)
    for h in range(2):
        total_arrival(h, 0).wait_recv()
        last_out[h] = (first[h, 1 - side] + ring_in[0, h, 1 - side].astype(jnp.float32)).astype(
            jnp.bfloat16
        )
        remote(
            last_out.at[h], last_in.at[h], l_send.at[h], l_recv.at[h], (me, other_side)
        ).start()
    for h in range(2):
        done = remote(last_out.at[h], last_in.at[h], l_send.at[h], l_recv.at[h], (me, other_side))
        done.wait_recv()
        out_ref[pl.ds(h * half, half), :] = (
            first[h, side] + ring_in[0, h, side].astype(jnp.float32) + last_in[h].astype(jnp.float32)
        )
        done.wait_send()
        side_copy(h).wait_send()

    def finish(step, carry):
        for h in range(2):
            core_copy(h, step).wait_send()

            @pl.when(step < n - 1)
            def _():
                ring_copy(h, step).wait_send()

            @pl.when(step > 0)
            def _():
                total_copy(h, step).wait_send()

        sums_copy(step).wait_send()
        return carry

    lax.fori_loop(0, n, finish, 0)


def flip(z, k, bits):
    out = 0
    for b in range(bits):
        zb = (z // (1 << b)) % 2
        kb = (k // (1 << b)) % 2
        out = out + (zb + kb - 2 * zb * kb) * (1 << b)
    return out


def remote(src, dst, send, recv, peer):
    return pltpu.make_async_remote_copy(
        src_ref=src, dst_ref=dst, send_sem=send, recv_sem=recv,
        device_id=peer, device_id_type=pl.DeviceIdType.MESH,
    )


def lanes_to_rows(row):
    return jnp.transpose(jnp.broadcast_to(row, (128, row.shape[1])))


def front_kernel(
    n, head, q_ref, kt_ref, vt_ref, qg_ref, kg_ref, ag_ref, res_ref, w_ref, fg_ref, rt_ref, rw_ref,
    cos_ref, sin_ref, x_out, mid_out, share_out,
    kv_all, q_all, m_s, l_s, acc, att_all, ss_all, sh_own, sh_all,
    z_send, kv_recv, y_send, sh_send, sh_recv, a_send, a_recv, s_send, s_recv,
):
    f32, bf16 = jnp.float32, jnp.bfloat16
    me = lax.axis_index("sp")
    tp = lax.axis_index("tp")
    core = tp % 2
    side = tp // 2
    other_core = side * 2 + 1 - core
    other_side = (1 - side) * 2 + core
    corner = (1 - side) * 2 + 1 - core
    nz = n // 2
    bits = nz.bit_length() - 1
    z = me // 2
    y = me % 2
    pair = 2 * z + 1 - y
    tokens = q_ref.shape[0]
    heads = q_ref.shape[1] // head
    quarter = head // 2

    barrier = pltpu.get_barrier_semaphore()
    for d in range(1, n):
        pl.semaphore_signal(
            barrier, inc=1, device_id=((me + d) % n, tp), device_id_type=pl.DeviceIdType.MESH
        )
    for peer in (other_core, other_side, corner):
        pl.semaphore_signal(
            barrier, inc=1, device_id=(me, peer), device_id_type=pl.DeviceIdType.MESH
        )

    cos_t = cos_ref[me]
    sin_t = sin_ref[me]
    key = kt_ref[...].astype(f32)
    gain_rows = lanes_to_rows(jnp.concatenate([kg_ref[...], kg_ref[...]], axis=1))[:head, :1]
    mean = jnp.sum(key * key, axis=0, keepdims=True) / head
    scaled = key * lax.rsqrt(mean + EPS) * gain_rows
    first, second = scaled[:quarter], scaled[quarter:]
    kv_all[me, :quarter, :] = (first * cos_t - second * sin_t).astype(bf16)
    kv_all[me, quarter:head, :] = (first * sin_t + second * cos_t).astype(bf16)
    kv_all[me, head:, :] = vt_ref[...]

    pl.semaphore_wait(barrier, n + 2)

    def z_copy(k):
        return remote(
            kv_all.at[me], kv_all.at[me], z_send.at[k], kv_recv.at[me],
            (2 * flip(z, k, bits) + y, tp),
        )

    def y_copy(k):
        block = 2 * flip(z, k, bits) + y
        return remote(
            kv_all.at[block], kv_all.at[block], y_send.at[k], kv_recv.at[block], (pair, tp)
        )

    def arrival(block):
        return remote(kv_all.at[block], kv_all.at[block], z_send.at[0], kv_recv.at[block], (pair, tp))

    y_copy(0).start()
    for k in range(1, nz):
        z_copy(k).start()

    chosen = jnp.zeros((sh_all.shape[0], tokens), f32)
    expert = lax.broadcasted_iota(jnp.int32, chosen.shape, 0)
    for k in range(rt_ref.shape[0]):
        chosen = chosen + jnp.where(expert == rt_ref[k : k + 1, :], rw_ref[k : k + 1, :], 0.0)
    for e in range(n):
        sh_own[e] = chosen[e : e + 1, :]

    def share_copy(d):
        to = (me + d) % n
        return remote(sh_own.at[to], sh_all.at[me], sh_send.at[d], sh_recv.at[me], (to, tp))

    def share_arrival(d):
        block = (me + n - d) % n
        return remote(sh_own.at[me], sh_all.at[block], sh_send.at[d], sh_recv.at[block], (block, tp))

    for d in range(1, n):
        share_copy(d).start()
    sh_all[me] = sh_own[me]

    cos_q = jnp.transpose(jnp.concatenate([cos_t] * 4, axis=0))
    sin_q = jnp.transpose(jnp.concatenate([-sin_t, sin_t] * 2, axis=0))
    lane = lax.broadcasted_iota(jnp.int32, (tokens, 128), 1)
    low = lane < head
    near = lane % head < quarter
    gain_q = jnp.concatenate([qg_ref[...], qg_ref[...]], axis=1)
    for j in range(heads // 2):
        x = q_ref[:, 128 * j : 128 * (j + 1)].astype(f32)
        square = x * x
        even = jnp.sum(jnp.where(low, square, 0.0), axis=1, keepdims=True)
        odd = jnp.sum(jnp.where(low, 0.0, square), axis=1, keepdims=True)
        inverse = lax.rsqrt(jnp.where(low, even, odd) / head + EPS)
        scaled = x * inverse * gain_q
        partner = jnp.where(
            near, pltpu.roll(scaled, 128 - quarter, 1), pltpu.roll(scaled, quarter, 1)
        )
        turned = (scaled * cos_q + partner * sin_q).astype(bf16).astype(f32) * (head**-0.5)
        q_all[2 * j] = jnp.where(low, turned, 0.0).astype(bf16)
        q_all[2 * j + 1] = jnp.where(low, 0.0, turned).astype(bf16)

    m_s[...] = jnp.full(m_s.shape, -1e30, f32)
    l_s[...] = jnp.zeros(l_s.shape, f32)
    acc[...] = jnp.zeros(acc.shape, f32)

    def group_step(k, carry):
        @pl.when(k < nz - 1)
        def _():
            arrival(2 * flip(z, k + 1, bits) + y).wait_recv()
            y_copy(k + 1).start()

        other = 2 * flip(z, k, bits) + 1 - y
        arrival(other).wait_recv()
        both = jnp.concatenate([kv_all[2 * flip(z, k, bits) + y], kv_all[other]], axis=1)
        kk = jnp.concatenate([both[:head], both[:head]], axis=0)
        vv = jnp.concatenate([both[head:], both[head:]], axis=0)
        pieces = both.shape[1] // 128
        for h in range(heads):
            scores = jnp.dot(q_all[h], kk, preferred_element_type=f32)
            old = m_s[h]
            new = jnp.maximum(old, jnp.max(scores, axis=1, keepdims=True))
            weights = jnp.exp(scores - jnp.concatenate([new] * pieces, axis=1))
            factor = jnp.exp(old - new)
            part = weights[:, :128]
            for i in range(1, pieces):
                part = part + weights[:, 128 * i : 128 * (i + 1)]
            l_s[h] = l_s[h] * factor + part
            acc[h] = acc[h] * factor + lax.dot_general(
                weights.astype(bf16), vv, (((1,), (1,)), ((), ())), preferred_element_type=f32
            )
            m_s[h] = new
        return carry

    lax.fori_loop(0, nz, group_step, 0)

    for j in range(heads // 2):
        even = acc[2 * j] / jnp.sum(l_s[2 * j], axis=1, keepdims=True)
        odd = acc[2 * j + 1] / jnp.sum(l_s[2 * j + 1], axis=1, keepdims=True)
        att_all[tp, :, 128 * j : 128 * (j + 1)] = jnp.where(low, even, odd).astype(bf16)

    def head_copy(i, slot, peer):
        return remote(att_all.at[slot], att_all.at[slot], a_send.at[i], a_recv.at[slot], (me, peer))

    head_copies = (
        head_copy(0, tp, other_side), head_copy(1, tp, other_core), head_copy(2, other_side, other_core)
    )
    head_copies[0].start()
    head_copies[1].start()
    for d in range(1, n):
        share_arrival(d).wait_recv()
    for b in range(n):
        share_out[b] = lanes_to_rows(sh_all[b])
    head_copy(0, other_side, other_side).wait_recv()
    head_copies[2].start()
    head_copy(1, other_core, other_core).wait_recv()
    head_copy(2, corner, other_core).wait_recv()

    every = jnp.concatenate([att_all[t] for t in range(4)], axis=1).astype(f32)
    mean = jnp.mean(every * every, axis=1, keepdims=True)
    normed = (every * lax.rsqrt(mean + EPS) * ag_ref[...]).astype(bf16)
    mid = (
        res_ref[...].astype(f32) + jnp.dot(normed, w_ref[...], preferred_element_type=f32)
    ).astype(bf16)
    mid_out[...] = mid
    mid_f = mid.astype(f32)
    square = mid_f * mid_f
    width = mid.shape[1]
    part = square[:, :128]
    for i in range(1, width // 128):
        part = part + square[:, 128 * i : 128 * (i + 1)]
    own = jnp.sum(jnp.transpose(part), axis=0, keepdims=True)
    ss_all[tp] = jnp.broadcast_to(own, ss_all.shape[1:])

    def sum_copy(i, slot, peer):
        return remote(ss_all.at[slot], ss_all.at[slot], s_send.at[i], s_recv.at[slot], (me, peer))

    peers = (other_side, corner, other_core)
    for i, peer in enumerate(peers):
        sum_copy(i, tp, peer).start()
    for i, peer in enumerate(peers):
        sum_copy(i, peer, peer).wait_recv()
    total = (ss_all[0] + ss_all[1]) + (ss_all[2] + ss_all[3])
    inverse = lax.rsqrt(lanes_to_rows(total[:1]) / (4 * width) + EPS)
    x_out[...] = (
        mid_f * jnp.concatenate([inverse] * (width // 128), axis=1) * fg_ref[...]
    ).astype(bf16)

    for k in range(nz):
        y_copy(k).wait_send()
    for k in range(1, nz):
        z_copy(k).wait_send()
    for d in range(1, n):
        share_copy(d).wait_send()
    for copy in head_copies:
        copy.wait_send()
    for i, peer in enumerate(peers):
        sum_copy(i, tp, peer).wait_send()


def front(args, n, head):
    (queries, keys, values, query_gain, key_norm_gain, attn_gain, residual, out_weight, ffn_gain,
     routes, route_weight) = args
    tokens, width = residual.shape
    heads = queries.shape[1] // head
    f32, bf16 = jnp.float32, jnp.bfloat16
    dma = pltpu.SemaphoreType.DMA
    vmem = pl.BlockSpec(memory_space=pltpu.VMEM)
    positions = np.arange(n * tokens)
    steps = np.float32(THETA) ** (-np.arange(0, head // 2, 2, dtype=np.float32) / np.float32(head // 2))
    angles = np.concatenate(
        [
            (positions // GRID_W).astype(np.float32)[:, None] * steps,
            (positions % GRID_W).astype(np.float32)[:, None] * steps,
        ],
        axis=1,
    ).reshape(n, tokens, head // 2).transpose(0, 2, 1)
    rows = max(8, n)
    return pl.pallas_call(
        functools.partial(front_kernel, n, head),
        out_shape=(
            jax.ShapeDtypeStruct((tokens, width), bf16),
            jax.ShapeDtypeStruct((tokens, width), bf16),
            jax.ShapeDtypeStruct((n, tokens, 128), f32),
        ),
        in_specs=[vmem] * 13,
        out_specs=(vmem, vmem, vmem),
        scratch_shapes=[
            pltpu.VMEM((n, 2 * head, tokens), bf16),
            pltpu.VMEM((heads, tokens, 128), bf16),
            pltpu.VMEM((heads, tokens, 128), f32),
            pltpu.VMEM((heads, tokens, 128), f32),
            pltpu.VMEM((heads, tokens, 128), f32),
            pltpu.VMEM((4, tokens, heads * head), bf16),
            pltpu.VMEM((4, 8, tokens), f32),
            pltpu.VMEM((rows, 1, tokens), f32),
            pltpu.VMEM((rows, 1, tokens), f32),
            dma((n // 2,)), dma((n,)), dma((n // 2,)), dma((n,)), dma((n,)),
            dma((3,)), dma((4,)), dma((3,)), dma((4,)),
        ],
        compiler_params=pltpu.CompilerParams(
            collective_id=1, has_side_effects=True, vmem_limit_bytes=60 * 1024 * 1024
        ),
    )(
        queries, keys.T, values.T, query_gain.reshape(1, head), key_norm_gain.reshape(1, head),
        attn_gain.reshape(1, -1), residual, out_weight, ffn_gain.reshape(1, -1),
        routes.T, route_weight.T,
        np.cos(angles).astype(np.float32), np.sin(angles).astype(np.float32),
    )


def exchange_and_compute(ffn_in, own_share, gate_weight, up_weight, down_weight, n):
    tokens, width = ffn_in.shape
    half = tokens // 2
    hidden = gate_weight.shape[2]
    full = gate_weight.shape[1]
    bf16, f32 = jnp.bfloat16, jnp.float32
    dma = pltpu.SemaphoreType.DMA
    vmem = pl.BlockSpec(memory_space=pltpu.VMEM)
    hbm = pl.BlockSpec(memory_space=pl.ANY)
    return pl.pallas_call(
        functools.partial(expert_kernel, n),
        out_shape=jax.ShapeDtypeStruct((tokens, width), f32),
        in_specs=[vmem, vmem, hbm, hbm, hbm],
        out_specs=vmem,
        scratch_shapes=[
            pltpu.VMEM((full, hidden), bf16),
            pltpu.VMEM((full, hidden), bf16),
            pltpu.VMEM((hidden, full), bf16),
            pltpu.VMEM((n, 2, 2, 2, half, width), bf16),
            pltpu.VMEM((n, 2, 2, half, width), bf16),
            pltpu.VMEM((n, 2, 2, half, width), bf16),
            pltpu.VMEM((n, 2, 2, half, width), bf16),
            pltpu.VMEM((n, 2, 2, half, width), bf16),
            pltpu.VMEM((2, 2, half, width), f32),
            pltpu.VMEM((2, 2, half, width), f32),
            pltpu.VMEM((2, half, width), bf16),
            pltpu.VMEM((2, half, width), bf16),
            dma((3,)), dma((2,)), dma((2,)), dma((2,)),
            dma((2, n)), dma((2, n)), dma((2, n)), dma((2, n)),
            dma((n,)), dma((n,)), dma((2, n)), dma((2, n)),
            dma((2,)), dma((2,)),
        ],
        compiler_params=pltpu.CompilerParams(
            collective_id=0, has_side_effects=True, vmem_limit_bytes=60 * 1024 * 1024
        ),
    )(ffn_in, own_share.reshape(n, 2, half, 128), gate_weight, up_weight, down_weight)


def per_device(
    queries,
    keys,
    values,
    query_gain,
    key_norm_gain,
    attn_gain,
    residual,
    out_weight,
    ffn_gain,
    routes,
    route_weight,
    gate_weight,
    up_weight,
    down_weight,
):
    tokens = queries.shape[0]
    head_size = query_gain.shape[0]
    experts = lax.axis_size("sp")
    paired = experts >= 4 and experts & (experts - 1) == 0 and experts <= 2 * routes.shape[1]
    if paired and lax.axis_size("tp") == 4 and keys.shape[1] == head_size == 64:
        ffn_in, mid_stream, share = front(
            (queries, keys, values, query_gain, key_norm_gain, attn_gain, residual, out_weight,
             ffn_gain, routes, route_weight),
            experts, head_size,
        )
        part = exchange_and_compute(ffn_in, share, gate_weight, up_weight, down_weight, experts)
        return (mid_stream.astype(jnp.float32) + part).astype(jnp.bfloat16)
    kv_local = keys.shape[1] // head_size
    q_local = queries.shape[1] // head_size
    group_width = q_local // kv_local
    first_token = lax.axis_index("sp") * tokens
    positions = first_token + jnp.arange(tokens, dtype=jnp.int32)
    cosine_lookup, sine_lookup = rotary_tables(positions, head_size, GRID_W)
    query_rotated = normalize_then_rotate(
        queries.reshape(tokens, q_local, head_size), query_gain, cosine_lookup, sine_lookup
    )
    key_rotated = normalize_then_rotate(
        keys.reshape(tokens, kv_local, head_size), key_norm_gain, cosine_lookup, sine_lookup
    )
    query_rows = query_rotated.reshape(tokens, kv_local, group_width, head_size).transpose(
        1, 0, 2, 3
    )
    query_rows = query_rows.reshape(kv_local, tokens * group_width, head_size)
    value_rows = values.reshape(tokens, kv_local, head_size)
    score_scale = head_size ** (-0.5)
    query_width = tokens * group_width
    start_state = (
        jnp.full((kv_local, query_width), -1e30, jnp.float32),
        jnp.zeros((kv_local, query_width), jnp.float32),
        jnp.zeros((kv_local, query_width, head_size), jnp.float32),
    )
    kv_width = kv_local * head_size
    packed = jnp.concatenate([key_rotated.reshape(tokens, kv_width), values], axis=1)
    gathered = lax.all_gather(packed, "sp", axis=0, tiled=True)
    piece_keys = gathered[:, :kv_width].reshape(-1, kv_local, head_size)
    piece_values = gathered[:, kv_width:].reshape(-1, kv_local, head_size)
    slot_count = piece_keys.shape[0]
    block_rows = 2048
    key_blocks = piece_keys.reshape(slot_count // block_rows, block_rows, kv_local, head_size)
    value_blocks = piece_values.reshape(slot_count // block_rows, block_rows, kv_local, head_size)

    def one_block(softmax_state, pair_block):
        running_max, running_sum, accumulated = softmax_state
        key_block, value_block = pair_block
        scores = (
            jnp.einsum("kqd,nkd->kqn", query_rows, key_block, preferred_element_type=jnp.float32)
            * score_scale
        )
        new_max = jnp.maximum(running_max, jnp.max(scores, axis=-1))
        weights = jnp.exp(scores - new_max[..., None])
        factor = jnp.exp(running_max - new_max)
        running_sum = running_sum * factor + jnp.sum(weights, axis=-1)
        accumulated = accumulated * factor[..., None] + jnp.einsum(
            "kqn,nkd->kqd",
            weights.astype(jnp.bfloat16),
            value_block,
            preferred_element_type=jnp.float32,
        )
        return ((new_max, running_sum, accumulated), None)

    final_state, unused_out = lax.scan(one_block, start_state, (key_blocks, value_blocks))
    running_max, running_sum, accumulated = final_state
    attended = (accumulated / running_sum[..., None]).reshape(
        kv_local, tokens, group_width, head_size
    )
    attended = (
        attended.transpose(1, 0, 2, 3).reshape(tokens, q_local * head_size).astype(jnp.bfloat16)
    )
    all_heads = lax.all_gather(attended, "tp", axis=1, tiled=True)
    head_f = all_heads.astype(jnp.float32)
    attn_normed = (
        head_f * lax.rsqrt(jnp.mean(head_f * head_f, axis=-1, keepdims=True) + EPS) * attn_gain
    ).astype(jnp.bfloat16)
    mid_stream = (
        residual.astype(jnp.float32)
        + jnp.dot(attn_normed, out_weight, preferred_element_type=jnp.float32)
    ).astype(jnp.bfloat16)
    mid_f = mid_stream.astype(jnp.float32)
    square_total = lax.psum(jnp.sum(mid_f * mid_f, axis=-1), "tp")
    ffn_in = (mid_f * lax.rsqrt(square_total / D + EPS)[:, None] * ffn_gain).astype(jnp.bfloat16)
    top_k = routes.shape[1]
    capacity = tokens * top_k * 3 // (2 * experts)
    route_list = routes.reshape(-1)
    onehot = (route_list[:, None] == jnp.arange(experts, dtype=jnp.int32)[None, :]).astype(
        jnp.int32
    )
    route_ranks = jnp.sum((jnp.cumsum(onehot, axis=0) - 1) * onehot, axis=1)
    slot_index = route_list * capacity + route_ranks
    slot_owner = (
        jnp.full((experts * capacity,), tokens, jnp.int32)
        .at[slot_index]
        .set(jnp.arange(tokens * top_k, dtype=jnp.int32) // top_k)
    )
    padded = jnp.concatenate([ffn_in, jnp.zeros((1, ffn_in.shape[1]), ffn_in.dtype)], axis=0)
    slot_block = lax.all_to_all(
        padded[slot_owner].reshape(experts, capacity, ffn_in.shape[1]),
        "sp",
        split_axis=0,
        concat_axis=0,
        tiled=True,
    )
    slot_count = slot_block.shape[1]
    slot_rows = slot_block.reshape(-1, slot_block.shape[2])
    column_piece = lax.all_gather(slot_rows, "tp", axis=1, tiled=True)
    gate_rows = gate_weight[0]
    up_rows = up_weight[0]
    gate_sum = jnp.dot(column_piece, gate_rows, preferred_element_type=jnp.float32)
    up_sum = jnp.dot(column_piece, up_rows, preferred_element_type=jnp.float32)
    partial_value = jnp.dot(
        clamped_unit(gate_sum, up_sum), down_weight[0], preferred_element_type=jnp.float32
    )
    summed = lax.psum_scatter(
        partial_value.astype(jnp.bfloat16), "tp", scatter_dimension=1, tiled=True
    )
    results = lax.all_to_all(
        summed.reshape(experts, slot_count, summed.shape[1]),
        "sp",
        split_axis=0,
        concat_axis=0,
        tiled=True,
    )
    picked = results.reshape(experts * capacity, -1)[slot_index].astype(jnp.float32)
    weighted = jnp.sum(
        (picked * route_weight.reshape(-1)[:, None]).reshape(tokens, top_k, -1), axis=1
    )
    return (mid_f + weighted).astype(jnp.bfloat16)


def solution(mesh):
    placed = (
        P("sp", "tp"),
        P("sp", "tp"),
        P("sp", "tp"),
        P(),
        P(),
        P(),
        P("sp", "tp"),
        P(None, "tp"),
        P("tp"),
        P("sp", None),
        P("sp", None),
        P("sp", None, "tp"),
        P("sp", None, "tp"),
        P("sp", "tp", None),
    )
    return jax.shard_map(
        per_device, mesh=mesh, in_specs=placed, out_specs=P("sp", "tp"), check_vma=False
    )
```

```python
import functools

import jax
import jax.numpy as jnp
import numpy as np
from jax import lax
from jax.experimental import pallas as pl
from jax.experimental.pallas import tpu as pltpu
from jax.sharding import PartitionSpec as P

D = 2048
GRID_W = 64


EPS = 1e-06
THETA = 10000.0
ALPHA = 1.702
LIMIT = 7.0
KEPT = 3


def rotary_tables(positions, head_size, grid_width):
    row_pos = (positions // grid_width).astype(jnp.float32)
    col_pos = (positions % grid_width).astype(jnp.float32)
    half_size = head_size // 2
    inverse = THETA ** (-jnp.arange(0, half_size, 2, dtype=jnp.float32) / half_size)
    angles = jnp.concatenate([row_pos[:, None] * inverse, col_pos[:, None] * inverse], axis=-1)
    return (jnp.cos(angles), jnp.sin(angles))


def normalize_then_rotate(head_rows, gain_vector, cosine_lookup, sine_lookup):
    values_f = head_rows.astype(jnp.float32)
    scaled = (
        values_f
        * lax.rsqrt(jnp.mean(values_f * values_f, axis=-1, keepdims=True) + EPS)
        * gain_vector
    )
    first_half, second_half = jnp.split(scaled, 2, axis=-1)
    cos_part = cosine_lookup[:, None, :]
    sin_part = sine_lookup[:, None, :]
    return jnp.concatenate(
        [
            first_half * cos_part - second_half * sin_part,
            first_half * sin_part + second_half * cos_part,
        ],
        axis=-1,
    ).astype(jnp.bfloat16)


def clamped_unit(gate_sum, up_sum):
    gate_sum = jnp.minimum(gate_sum, LIMIT)
    up_sum = jnp.clip(up_sum, -LIMIT, LIMIT)
    return ((up_sum + 1.0) * gate_sum * jax.nn.sigmoid(ALPHA * gate_sum)).astype(jnp.bfloat16)


def ring_place(device, n):
    odd = lax.rem(device, 2)
    far = device // 2
    return (1 - odd) * far + odd * (n - 1 - far)


def ring_device(place, n):
    odd = place // (n // 2)
    return 2 * ((1 - odd) * place + odd * (n - 1 - place)) + odd


def expert_phase(
    n, kept_rows, held, gate_ref, up_ref, down_ref, share_ref, mid_ref, out_ref,
    core_out, core_in, sum_out, sum_in, ring_in, ring_out, kept, last_out, last_in,
    f_send, f_recv, x_send, x_recv, g_send, g_recv, c_send, c_recv,
    cs_send, cs_recv, xs_send, xs_recv, r_send, r_recv, l_send, l_recv,
):
    f32, bf16 = jnp.float32, jnp.bfloat16
    me = lax.axis_index("sp")
    tp = lax.axis_index("tp")
    core = lax.rem(tp, 2)
    side = tp // 2
    place = ring_place(me, n)
    targets = (ring_device(lax.rem(place + 1, n), n), ring_device(lax.rem(place + n - 1, n), n))
    other_core = side * 2 + 1 - core
    other_side = (1 - side) * 2 + core
    half = held.shape[4]
    width = held.shape[5]
    rest = half - kept_rows
    tail = pl.ds(kept_rows, rest)
    head = pl.ds(0, kept_rows)
    block_parts = ((0, tail), (0, head), (1, head))
    total_parts = ((0, head), (1, head), (0, tail))

    def owner(h, step):
        return ring_device(lax.rem(place + (n - step if h == 0 else step), n), n)

    def side_of(which):
        return side if which == 0 else 1 - side

    def first_copy(h):
        block = held.at[me, h, core, side, head]
        return remote(block, block, f_send.at[h], f_recv.at[h], (me, other_side))

    def first_arrival(h):
        block = held.at[me, h, core, 1 - side, head]
        return remote(block, block, f_send.at[h], f_recv.at[h], (me, other_side))

    def side_copy(h, step):
        block = held.at[owner(h, step), h, core, side, tail]
        return remote(block, block, x_send.at[h, step], x_recv.at[h, step], (me, other_side))

    def side_arrival(h, step):
        block = held.at[owner(h, step), h, core, 1 - side, tail]
        return remote(block, block, x_send.at[h, step], x_recv.at[h, step], (me, other_side))

    def ring_copy(h, step, i):
        which, rows = block_parts[i]
        block = held.at[owner(h, step), h, core, side_of(which), rows]
        return remote(
            block, block, g_send.at[h, i, step], g_recv.at[h, i, step + 1], (targets[h], tp)
        )

    def ring_arrival(h, step, i):
        which, rows = block_parts[i]
        block = held.at[owner(h, step), h, core, side_of(which), rows]
        return remote(block, block, g_send.at[h, i, step], g_recv.at[h, i, step], (targets[h], tp))

    def core_copy(which, h, step):
        block = held.at[owner(h, step), h, core, side_of(which)]
        return remote(
            block, block, c_send.at[which, h, step], c_recv.at[which, h, step], (me, other_core)
        )

    def core_arrival(which, h, step):
        block = held.at[owner(h, step), h, 1 - core, side_of(which)]
        return remote(
            block, block, c_send.at[which, h, step], c_recv.at[which, h, step], (me, other_core)
        )

    def core_sums(which, step):
        return remote(
            core_out.at[step, which], core_in.at[step, which],
            cs_send.at[which, step], cs_recv.at[which, step], (me, other_core),
        )

    def side_sums(h, step):
        return remote(
            sum_out.at[step, h], sum_in.at[step, h],
            xs_send.at[h, step], xs_recv.at[h, step], (me, other_side),
        )

    def total_copy(h, step, i):
        which, rows = total_parts[i]
        later = lax.rem(step + 1, n)
        return remote(
            ring_out.at[step, h, which, rows], ring_in.at[later, h, which, rows],
            r_send.at[h, i, step], r_recv.at[h, i, later], (targets[h], tp),
        )

    def total_arrival(h, step, i):
        which, rows = total_parts[i]
        return remote(
            ring_out.at[step, h, which, rows], ring_in.at[step, h, which, rows],
            r_send.at[h, i, step], r_recv.at[h, i, step], (targets[h], tp),
        )

    def last_copy(h):
        return remote(last_out.at[h], last_in.at[h], l_send.at[h], l_recv.at[h], (me, other_side))

    for h in range(2):
        first_copy(h).start()
    ring_in[1] = jnp.zeros(ring_in.shape[1:], bf16)

    def pass_on(step):
        for i in range(3):
            for h in range(2):
                @pl.when(step > 0)
                def _():
                    ring_arrival(h, step, i).wait_recv()

                if i == 2:
                    @pl.when(step == 0)
                    def _():
                        first_arrival(h).wait_recv()

                @pl.when(step < n - 1)
                def _():
                    ring_copy(h, step, i).start()

                if i == 0:
                    side_copy(h, step).start()
                if i == 1:
                    core_copy(0, h, step).start()

    def share_sides(step):
        for h in range(2):
            side_arrival(h, step).wait_recv()
            core_copy(1, h, step).start()

    def compute(step):
        now = lax.rem(step, 2)
        for h in range(2):
            for which in range(2):
                core_arrival(which, h, step).wait_recv()
        owners = (owner(0, step), owner(1, step))
        rows = jnp.concatenate(
            [
                jnp.concatenate([held[owners[h], h, t % 2, t // 2] for t in range(4)], axis=1)
                for h in range(2)
            ],
            axis=0,
        )
        gate_sum = jnp.dot(rows, gate_ref[...], preferred_element_type=f32)
        up_sum = jnp.dot(rows, up_ref[...], preferred_element_type=f32)
        units = clamped_unit(gate_sum, up_sum)
        share = jnp.concatenate(
            [share_ref[owners[h], h * half : (h + 1) * half] for h in range(2)], axis=0
        )
        share = jnp.concatenate([share] * (width // 128), axis=1)

        def part_of(c, which):
            columns = pl.ds(pl.multiple_of((2 * side_of(which) + c) * width, width), width)
            return jnp.dot(units, down_ref[:, columns], preferred_element_type=f32) * share

        for which in (1, 0):
            core_out[step, which] = part_of(1 - core, which).astype(bf16)
            core_sums(which, step).start()
        for which in (1, 0):
            kept[now, which] = part_of(core, which)

    def totals(step):
        now = lax.rem(step, 2)
        for i, (which, rows) in enumerate(total_parts):
            for h in range(2):
                start = h * half + rows.start
                value = kept[now, which, start : start + rows.size]
                if which == 0 and rows.start > 0:
                    side_sums(h, step).wait_recv()
                    value = value + sum_in[step, h].astype(f32)

                @pl.when(step > 1)
                def _():
                    total_arrival(h, step, i).wait_recv()

                ring_out[step, h, which, rows] = (
                    value + ring_in[step, h, which, rows].astype(f32)
                ).astype(bf16)
                total_copy(h, step, i).start()

    def pair_sums(step):
        now = lax.rem(step, 2)
        for which in (1, 0):
            core_sums(which, step).wait_recv()
            value = kept[now, which] + core_in[step, which].astype(f32)
            if which == 1:
                for h in range(2):
                    sum_out[step, h] = value[h * half + kept_rows : (h + 1) * half].astype(bf16)
                    side_sums(h, step).start()
            kept[now, which] = value

    def one_step(i, carry):
        @pl.when(i < n)
        def _():
            pass_on(i)

        @pl.when((i >= 1) & (i <= n))
        def _():
            share_sides(i - 1)

        last = i // (n + 2)
        busy = ((i >= 2) & (i <= n)) | (i == n + 2)
        block = (i - 1) * (1 - last)

        @pl.when(busy)
        def _():
            compute(block)

        @pl.when((i >= 3) & (i <= n + 1))
        def _():
            totals(i - 2)

        @pl.when(busy)
        def _():
            pair_sums(block)

        return carry

    lax.fori_loop(0, n + 3, one_step, 0)
    for h in range(2):
        rows = pl.ds(h * half, kept_rows)
        total_arrival(h, 0, 1).wait_recv()
        last_out[h] = (kept[0, 1, rows] + ring_in[0, h, 1, head].astype(f32)).astype(bf16)
        last_copy(h).start()
    for h in range(2):
        rows = pl.ds(h * half + kept_rows, rest)
        total_arrival(h, 0, 2).wait_recv()
        side_sums(h, 0).wait_recv()
        value = kept[0, 0, rows] + ring_in[0, h, 0, tail].astype(f32) + sum_in[0, h].astype(f32)
        out_ref[rows, :] = (mid_ref[rows, :].astype(f32) + value).astype(bf16)
    for h in range(2):
        rows = pl.ds(h * half, kept_rows)
        total_arrival(h, 0, 0).wait_recv()
        last_copy(h).wait_recv()
        value = kept[0, 0, rows] + ring_in[0, h, 0, head].astype(f32) + last_in[h].astype(f32)
        out_ref[rows, :] = (mid_ref[rows, :].astype(f32) + value).astype(bf16)
        first_copy(h).wait_send()
        last_copy(h).wait_send()

    def finish(step, carry):
        for h in range(2):
            side_copy(h, step).wait_send()
            side_sums(h, step).wait_send()
            core_sums(h, step).wait_send()
            for which in range(2):
                core_copy(which, h, step).wait_send()
            for i in range(3):
                @pl.when(step < n - 1)
                def _():
                    ring_copy(h, step, i).wait_send()

                @pl.when(step > 0)
                def _():
                    total_copy(h, step, i).wait_send()

        return carry

    lax.fori_loop(0, n, finish, 0)


def flip(z, k, bits):
    out = 0
    for b in range(bits):
        zb = (z // (1 << b)) % 2
        kb = (k // (1 << b)) % 2
        out = out + (zb + kb - 2 * zb * kb) * (1 << b)
    return out


def remote(src, dst, send, recv, peer):
    return pltpu.make_async_remote_copy(
        src_ref=src, dst_ref=dst, send_sem=send, recv_sem=recv,
        device_id=peer, device_id_type=pl.DeviceIdType.MESH,
    )


def lanes_to_rows(row):
    return jnp.transpose(jnp.broadcast_to(row, (128, row.shape[1])))


def layer_kernel(
    n, head, kept_rows, q_ref, kt_ref, vt_ref, qg_ref, kg_ref, ag_ref, res_ref, w_ref, fg_ref, rt_ref,
    rw_ref, cos_ref, sin_ref, gate_hbm, up_hbm, down_hbm, out_ref,
    gate_ref, up_ref, down_ref, held, mid_ref, share_ref, w_sem,
    kv_all, q_all, m_s, l_s, acc, att_all, ss_all, sh_own, sh_all,
    z_send, kv_recv, y_send, sh_send, sh_recv, a_send, a_recv, s_send, s_recv,
    *expert_refs,
):
    f32, bf16 = jnp.float32, jnp.bfloat16
    loads = [
        pltpu.make_async_copy(src.at[0], dst, w_sem.at[i])
        for i, (src, dst) in enumerate(((gate_hbm, gate_ref), (up_hbm, up_ref), (down_hbm, down_ref)))
    ]
    for load in loads:
        load.start()
    me = lax.axis_index("sp")
    tp = lax.axis_index("tp")
    core = tp % 2
    side = tp // 2
    other_core = side * 2 + 1 - core
    other_side = (1 - side) * 2 + core
    corner = (1 - side) * 2 + 1 - core
    nz = n // 2
    bits = nz.bit_length() - 1
    z = me // 2
    y = me % 2
    pair = 2 * z + 1 - y
    tokens = q_ref.shape[0]
    heads = q_ref.shape[1] // head
    quarter = head // 2

    barrier = pltpu.get_barrier_semaphore()
    for d in range(1, n):
        pl.semaphore_signal(
            barrier, inc=1, device_id=((me + d) % n, tp), device_id_type=pl.DeviceIdType.MESH
        )
    for peer in (other_core, other_side, corner):
        pl.semaphore_signal(
            barrier, inc=1, device_id=(me, peer), device_id_type=pl.DeviceIdType.MESH
        )

    cos_t = cos_ref[me]
    sin_t = sin_ref[me]
    key = kt_ref[...].astype(f32)
    gain_rows = lanes_to_rows(jnp.concatenate([kg_ref[...], kg_ref[...]], axis=1))[:head, :1]
    mean = jnp.sum(key * key, axis=0, keepdims=True) / head
    scaled = key * lax.rsqrt(mean + EPS) * gain_rows
    first, second = scaled[:quarter], scaled[quarter:]
    kv_all[me, :quarter, :] = (first * cos_t - second * sin_t).astype(bf16)
    kv_all[me, quarter:head, :] = (first * sin_t + second * cos_t).astype(bf16)
    kv_all[me, head:, :] = vt_ref[...]

    pl.semaphore_wait(barrier, n + 2)

    def z_copy(k):
        return remote(
            kv_all.at[me], kv_all.at[me], z_send.at[k], kv_recv.at[me],
            (2 * flip(z, k, bits) + y, tp),
        )

    def y_copy(k):
        block = 2 * flip(z, k, bits) + y
        return remote(
            kv_all.at[block], kv_all.at[block], y_send.at[k], kv_recv.at[block], (pair, tp)
        )

    def arrival(block):
        return remote(kv_all.at[block], kv_all.at[block], z_send.at[0], kv_recv.at[block], (pair, tp))

    y_copy(0).start()
    for k in range(1, nz):
        z_copy(k).start()

    chosen = jnp.zeros((sh_all.shape[0], tokens), f32)
    expert = lax.broadcasted_iota(jnp.int32, chosen.shape, 0)
    for k in range(rt_ref.shape[0]):
        chosen = chosen + jnp.where(expert == rt_ref[k : k + 1, :], rw_ref[k : k + 1, :], 0.0)
    for e in range(n):
        sh_own[e] = chosen[e : e + 1, :]

    def share_copy(d):
        to = (me + d) % n
        return remote(sh_own.at[to], sh_all.at[me], sh_send.at[d], sh_recv.at[me], (to, tp))

    def share_arrival(d):
        block = (me + n - d) % n
        return remote(sh_own.at[me], sh_all.at[block], sh_send.at[d], sh_recv.at[block], (block, tp))

    for d in range(1, n):
        share_copy(d).start()
    sh_all[me] = sh_own[me]

    cos_q = jnp.transpose(jnp.concatenate([cos_t] * 4, axis=0))
    sin_q = jnp.transpose(jnp.concatenate([-sin_t, sin_t] * 2, axis=0))
    lane = lax.broadcasted_iota(jnp.int32, (tokens, 128), 1)
    low = lane < head
    near = lane % head < quarter
    gain_q = jnp.concatenate([qg_ref[...], qg_ref[...]], axis=1)
    for j in range(heads // 2):
        x = q_ref[:, 128 * j : 128 * (j + 1)].astype(f32)
        square = x * x
        even = jnp.sum(jnp.where(low, square, 0.0), axis=1, keepdims=True)
        odd = jnp.sum(jnp.where(low, 0.0, square), axis=1, keepdims=True)
        inverse = lax.rsqrt(jnp.where(low, even, odd) / head + EPS)
        scaled = x * inverse * gain_q
        partner = jnp.where(
            near, pltpu.roll(scaled, 128 - quarter, 1), pltpu.roll(scaled, quarter, 1)
        )
        turned = (scaled * cos_q + partner * sin_q).astype(bf16).astype(f32) * (head**-0.5)
        q_all[2 * j] = jnp.where(low, turned, 0.0).astype(bf16)
        q_all[2 * j + 1] = jnp.where(low, 0.0, turned).astype(bf16)

    m_s[...] = jnp.full(m_s.shape, -1e30, f32)
    l_s[...] = jnp.zeros(l_s.shape, f32)
    acc[...] = jnp.zeros(acc.shape, f32)

    def group_step(k, carry):
        @pl.when(k < nz - 1)
        def _():
            arrival(2 * flip(z, k + 1, bits) + y).wait_recv()
            y_copy(k + 1).start()

        other = 2 * flip(z, k, bits) + 1 - y
        arrival(other).wait_recv()
        both = jnp.concatenate([kv_all[2 * flip(z, k, bits) + y], kv_all[other]], axis=1)
        kk = jnp.concatenate([both[:head], both[:head]], axis=0)
        vv = jnp.concatenate([both[head:], both[head:]], axis=0)
        pieces = both.shape[1] // 128
        for h in range(heads):
            scores = jnp.dot(q_all[h], kk, preferred_element_type=f32)
            old = m_s[h]
            new = jnp.maximum(old, jnp.max(scores, axis=1, keepdims=True))
            weights = jnp.exp(scores - jnp.concatenate([new] * pieces, axis=1))
            factor = jnp.exp(old - new)
            part = weights[:, :128]
            for i in range(1, pieces):
                part = part + weights[:, 128 * i : 128 * (i + 1)]
            l_s[h] = l_s[h] * factor + part
            acc[h] = acc[h] * factor + lax.dot_general(
                weights.astype(bf16), vv, (((1,), (1,)), ((), ())), preferred_element_type=f32
            )
            m_s[h] = new
        return carry

    lax.fori_loop(0, nz, group_step, 0)

    for j in range(heads // 2):
        even = acc[2 * j] / jnp.sum(l_s[2 * j], axis=1, keepdims=True)
        odd = acc[2 * j + 1] / jnp.sum(l_s[2 * j + 1], axis=1, keepdims=True)
        att_all[tp, :, 128 * j : 128 * (j + 1)] = jnp.where(low, even, odd).astype(bf16)

    def head_copy(i, slot, peer):
        return remote(att_all.at[slot], att_all.at[slot], a_send.at[i], a_recv.at[slot], (me, peer))

    head_copies = (
        head_copy(0, tp, other_side), head_copy(1, tp, other_core), head_copy(2, other_side, other_core)
    )
    head_copies[0].start()
    head_copies[1].start()
    for d in range(1, n):
        share_arrival(d).wait_recv()
    for b in range(n):
        share_ref[b] = lanes_to_rows(sh_all[b])
    head_copy(0, other_side, other_side).wait_recv()
    head_copies[2].start()
    head_copy(1, other_core, other_core).wait_recv()
    head_copy(2, corner, other_core).wait_recv()

    every = jnp.concatenate([att_all[t] for t in range(4)], axis=1).astype(f32)
    mean = jnp.mean(every * every, axis=1, keepdims=True)
    normed = (every * lax.rsqrt(mean + EPS) * ag_ref[...]).astype(bf16)
    mid = (
        res_ref[...].astype(f32) + jnp.dot(normed, w_ref[...], preferred_element_type=f32)
    ).astype(bf16)
    mid_ref[...] = mid
    mid_f = mid.astype(f32)
    square = mid_f * mid_f
    width = mid.shape[1]
    part = square[:, :128]
    for i in range(1, width // 128):
        part = part + square[:, 128 * i : 128 * (i + 1)]
    own = jnp.sum(jnp.transpose(part), axis=0, keepdims=True)
    ss_all[tp] = jnp.broadcast_to(own, ss_all.shape[1:])

    def sum_copy(i, slot, peer):
        return remote(ss_all.at[slot], ss_all.at[slot], s_send.at[i], s_recv.at[slot], (me, peer))

    peers = (other_side, corner, other_core)
    for i, peer in enumerate(peers):
        sum_copy(i, tp, peer).start()
    for i, peer in enumerate(peers):
        sum_copy(i, peer, peer).wait_recv()
    total = (ss_all[0] + ss_all[1]) + (ss_all[2] + ss_all[3])
    inverse = lax.rsqrt(lanes_to_rows(total[:1]) / (4 * width) + EPS)
    ffn_in = (
        mid_f * jnp.concatenate([inverse] * (width // 128), axis=1) * fg_ref[...]
    ).astype(bf16)
    half = tokens // 2
    for h in range(2):
        held[me, h, core, side] = ffn_in[h * half : (h + 1) * half]
    for load in loads:
        load.wait()
    expert_phase(
        n, kept_rows, held, gate_ref, up_ref, down_ref, share_ref, mid_ref, out_ref, *expert_refs
    )

    for k in range(nz):
        y_copy(k).wait_send()
    for k in range(1, nz):
        z_copy(k).wait_send()
    for d in range(1, n):
        share_copy(d).wait_send()
    for copy in head_copies:
        copy.wait_send()
    for i, peer in enumerate(peers):
        sum_copy(i, tp, peer).wait_send()


def whole_layer(args, n, head):
    (queries, keys, values, query_gain, key_norm_gain, attn_gain, residual, out_weight, ffn_gain,
     routes, route_weight, gate_weight, up_weight, down_weight) = args
    tokens, width = residual.shape
    full, hidden = gate_weight.shape[1:]
    half = tokens // 2
    kept_rows = KEPT * half // 8
    rest = half - kept_rows
    hbm = pl.BlockSpec(memory_space=pl.ANY)
    heads = queries.shape[1] // head
    f32, bf16 = jnp.float32, jnp.bfloat16
    dma = pltpu.SemaphoreType.DMA
    vmem = pl.BlockSpec(memory_space=pltpu.VMEM)
    positions = np.arange(n * tokens)
    steps = np.float32(THETA) ** (-np.arange(0, head // 2, 2, dtype=np.float32) / np.float32(head // 2))
    angles = np.concatenate(
        [
            (positions // GRID_W).astype(np.float32)[:, None] * steps,
            (positions % GRID_W).astype(np.float32)[:, None] * steps,
        ],
        axis=1,
    ).reshape(n, tokens, head // 2).transpose(0, 2, 1)
    rows = max(8, n)
    return pl.pallas_call(
        functools.partial(layer_kernel, n, head, kept_rows),
        out_shape=jax.ShapeDtypeStruct((tokens, width), bf16),
        in_specs=[vmem] * 13 + [hbm] * 3,
        out_specs=vmem,
        scratch_shapes=[
            pltpu.VMEM((full, hidden), bf16),
            pltpu.VMEM((full, hidden), bf16),
            pltpu.VMEM((hidden, full), bf16),
            pltpu.VMEM((n, 2, 2, 2, half, width), bf16),
            pltpu.VMEM((tokens, width), bf16),
            pltpu.VMEM((n, tokens, 128), f32),
            dma((3,)),
            pltpu.VMEM((n, 2 * head, tokens), bf16),
            pltpu.VMEM((heads, tokens, 128), bf16),
            pltpu.VMEM((heads, tokens, 128), f32),
            pltpu.VMEM((heads, tokens, 128), f32),
            pltpu.VMEM((heads, tokens, 128), f32),
            pltpu.VMEM((4, tokens, heads * head), bf16),
            pltpu.VMEM((4, 8, tokens), f32),
            pltpu.VMEM((rows, 1, tokens), f32),
            pltpu.VMEM((rows, 1, tokens), f32),
            dma((n // 2,)), dma((n,)), dma((n // 2,)), dma((n,)), dma((n,)),
            dma((3,)), dma((4,)), dma((3,)), dma((4,)),
            pltpu.VMEM((n, 2, tokens, width), bf16),
            pltpu.VMEM((n, 2, tokens, width), bf16),
            pltpu.VMEM((n, 2, rest, width), bf16),
            pltpu.VMEM((n, 2, rest, width), bf16),
            pltpu.VMEM((n, 2, 2, half, width), bf16),
            pltpu.VMEM((n, 2, 2, half, width), bf16),
            pltpu.VMEM((2, 2, tokens, width), f32),
            pltpu.VMEM((2, kept_rows, width), bf16),
            pltpu.VMEM((2, kept_rows, width), bf16),
            dma((2,)), dma((2,)), dma((2, n)), dma((2, n)),
            dma((2, 3, n)), dma((2, 3, n)), dma((2, 2, n)), dma((2, 2, n)),
            dma((2, n)), dma((2, n)), dma((2, n)), dma((2, n)),
            dma((2, 3, n)), dma((2, 3, n)), dma((2,)), dma((2,)),
        ],
        compiler_params=pltpu.CompilerParams(
            collective_id=0, has_side_effects=True, vmem_limit_bytes=60 * 1024 * 1024
        ),
    )(
        queries, keys.T, values.T, query_gain.reshape(1, head), key_norm_gain.reshape(1, head),
        attn_gain.reshape(1, -1), residual, out_weight, ffn_gain.reshape(1, -1),
        routes.T, route_weight.T,
        np.cos(angles).astype(np.float32), np.sin(angles).astype(np.float32),
        gate_weight, up_weight, down_weight,
    )


def per_device(
    queries,
    keys,
    values,
    query_gain,
    key_norm_gain,
    attn_gain,
    residual,
    out_weight,
    ffn_gain,
    routes,
    route_weight,
    gate_weight,
    up_weight,
    down_weight,
):
    tokens = queries.shape[0]
    head_size = query_gain.shape[0]
    experts = lax.axis_size("sp")
    paired = experts >= 4 and experts & (experts - 1) == 0 and experts <= 2 * routes.shape[1]
    if paired and lax.axis_size("tp") == 4 and keys.shape[1] == head_size == 64:
        return whole_layer(
            (queries, keys, values, query_gain, key_norm_gain, attn_gain, residual, out_weight,
             ffn_gain, routes, route_weight, gate_weight, up_weight, down_weight),
            experts, head_size,
        )
    kv_local = keys.shape[1] // head_size
    q_local = queries.shape[1] // head_size
    group_width = q_local // kv_local
    first_token = lax.axis_index("sp") * tokens
    positions = first_token + jnp.arange(tokens, dtype=jnp.int32)
    cosine_lookup, sine_lookup = rotary_tables(positions, head_size, GRID_W)
    query_rotated = normalize_then_rotate(
        queries.reshape(tokens, q_local, head_size), query_gain, cosine_lookup, sine_lookup
    )
    key_rotated = normalize_then_rotate(
        keys.reshape(tokens, kv_local, head_size), key_norm_gain, cosine_lookup, sine_lookup
    )
    query_rows = query_rotated.reshape(tokens, kv_local, group_width, head_size).transpose(
        1, 0, 2, 3
    )
    query_rows = query_rows.reshape(kv_local, tokens * group_width, head_size)
    value_rows = values.reshape(tokens, kv_local, head_size)
    score_scale = head_size ** (-0.5)
    query_width = tokens * group_width
    start_state = (
        jnp.full((kv_local, query_width), -1e30, jnp.float32),
        jnp.zeros((kv_local, query_width), jnp.float32),
        jnp.zeros((kv_local, query_width, head_size), jnp.float32),
    )
    kv_width = kv_local * head_size
    packed = jnp.concatenate([key_rotated.reshape(tokens, kv_width), values], axis=1)
    gathered = lax.all_gather(packed, "sp", axis=0, tiled=True)
    piece_keys = gathered[:, :kv_width].reshape(-1, kv_local, head_size)
    piece_values = gathered[:, kv_width:].reshape(-1, kv_local, head_size)
    slot_count = piece_keys.shape[0]
    block_rows = 2048
    key_blocks = piece_keys.reshape(slot_count // block_rows, block_rows, kv_local, head_size)
    value_blocks = piece_values.reshape(slot_count // block_rows, block_rows, kv_local, head_size)

    def one_block(softmax_state, pair_block):
        running_max, running_sum, accumulated = softmax_state
        key_block, value_block = pair_block
        scores = (
            jnp.einsum("kqd,nkd->kqn", query_rows, key_block, preferred_element_type=jnp.float32)
            * score_scale
        )
        new_max = jnp.maximum(running_max, jnp.max(scores, axis=-1))
        weights = jnp.exp(scores - new_max[..., None])
        factor = jnp.exp(running_max - new_max)
        running_sum = running_sum * factor + jnp.sum(weights, axis=-1)
        accumulated = accumulated * factor[..., None] + jnp.einsum(
            "kqn,nkd->kqd",
            weights.astype(jnp.bfloat16),
            value_block,
            preferred_element_type=jnp.float32,
        )
        return ((new_max, running_sum, accumulated), None)

    final_state, unused_out = lax.scan(one_block, start_state, (key_blocks, value_blocks))
    running_max, running_sum, accumulated = final_state
    attended = (accumulated / running_sum[..., None]).reshape(
        kv_local, tokens, group_width, head_size
    )
    attended = (
        attended.transpose(1, 0, 2, 3).reshape(tokens, q_local * head_size).astype(jnp.bfloat16)
    )
    all_heads = lax.all_gather(attended, "tp", axis=1, tiled=True)
    head_f = all_heads.astype(jnp.float32)
    attn_normed = (
        head_f * lax.rsqrt(jnp.mean(head_f * head_f, axis=-1, keepdims=True) + EPS) * attn_gain
    ).astype(jnp.bfloat16)
    mid_stream = (
        residual.astype(jnp.float32)
        + jnp.dot(attn_normed, out_weight, preferred_element_type=jnp.float32)
    ).astype(jnp.bfloat16)
    mid_f = mid_stream.astype(jnp.float32)
    square_total = lax.psum(jnp.sum(mid_f * mid_f, axis=-1), "tp")
    ffn_in = (mid_f * lax.rsqrt(square_total / D + EPS)[:, None] * ffn_gain).astype(jnp.bfloat16)
    top_k = routes.shape[1]
    capacity = tokens * top_k * 3 // (2 * experts)
    route_list = routes.reshape(-1)
    onehot = (route_list[:, None] == jnp.arange(experts, dtype=jnp.int32)[None, :]).astype(
        jnp.int32
    )
    route_ranks = jnp.sum((jnp.cumsum(onehot, axis=0) - 1) * onehot, axis=1)
    slot_index = route_list * capacity + route_ranks
    slot_owner = (
        jnp.full((experts * capacity,), tokens, jnp.int32)
        .at[slot_index]
        .set(jnp.arange(tokens * top_k, dtype=jnp.int32) // top_k)
    )
    padded = jnp.concatenate([ffn_in, jnp.zeros((1, ffn_in.shape[1]), ffn_in.dtype)], axis=0)
    slot_block = lax.all_to_all(
        padded[slot_owner].reshape(experts, capacity, ffn_in.shape[1]),
        "sp",
        split_axis=0,
        concat_axis=0,
        tiled=True,
    )
    slot_count = slot_block.shape[1]
    slot_rows = slot_block.reshape(-1, slot_block.shape[2])
    column_piece = lax.all_gather(slot_rows, "tp", axis=1, tiled=True)
    gate_rows = gate_weight[0]
    up_rows = up_weight[0]
    gate_sum = jnp.dot(column_piece, gate_rows, preferred_element_type=jnp.float32)
    up_sum = jnp.dot(column_piece, up_rows, preferred_element_type=jnp.float32)
    partial_value = jnp.dot(
        clamped_unit(gate_sum, up_sum), down_weight[0], preferred_element_type=jnp.float32
    )
    summed = lax.psum_scatter(
        partial_value.astype(jnp.bfloat16), "tp", scatter_dimension=1, tiled=True
    )
    results = lax.all_to_all(
        summed.reshape(experts, slot_count, summed.shape[1]),
        "sp",
        split_axis=0,
        concat_axis=0,
        tiled=True,
    )
    picked = results.reshape(experts * capacity, -1)[slot_index].astype(jnp.float32)
    weighted = jnp.sum(
        (picked * route_weight.reshape(-1)[:, None]).reshape(tokens, top_k, -1), axis=1
    )
    return (mid_f + weighted).astype(jnp.bfloat16)


def solution(mesh):
    placed = (
        P("sp", "tp"),
        P("sp", "tp"),
        P("sp", "tp"),
        P(),
        P(),
        P(),
        P("sp", "tp"),
        P(None, "tp"),
        P("tp"),
        P("sp", None),
        P("sp", None),
        P("sp", None, "tp"),
        P("sp", None, "tp"),
        P("sp", "tp", None),
    )
    return jax.shard_map(
        per_device, mesh=mesh, in_specs=placed, out_specs=P("sp", "tp"), check_vma=False
    )
```

```python
import functools

import jax
import jax.numpy as jnp
import numpy as np
from jax import lax
from jax.experimental import pallas as pl
from jax.experimental.pallas import tpu as pltpu
from jax.sharding import PartitionSpec as P

D = 2048
GRID_W = 64


EPS = 1e-06
THETA = 10000.0
ALPHA = 1.702
LIMIT = 7.0
BLOCK_ROWS = 4
TOTAL_ROWS = 3


def rotary_tables(positions, head_size, grid_width):
    row_pos = (positions // grid_width).astype(jnp.float32)
    col_pos = (positions % grid_width).astype(jnp.float32)
    half_size = head_size // 2
    inverse = THETA ** (-jnp.arange(0, half_size, 2, dtype=jnp.float32) / half_size)
    angles = jnp.concatenate([row_pos[:, None] * inverse, col_pos[:, None] * inverse], axis=-1)
    return (jnp.cos(angles), jnp.sin(angles))


def normalize_then_rotate(head_rows, gain_vector, cosine_lookup, sine_lookup):
    values_f = head_rows.astype(jnp.float32)
    scaled = (
        values_f
        * lax.rsqrt(jnp.mean(values_f * values_f, axis=-1, keepdims=True) + EPS)
        * gain_vector
    )
    first_half, second_half = jnp.split(scaled, 2, axis=-1)
    cos_part = cosine_lookup[:, None, :]
    sin_part = sine_lookup[:, None, :]
    return jnp.concatenate(
        [
            first_half * cos_part - second_half * sin_part,
            first_half * sin_part + second_half * cos_part,
        ],
        axis=-1,
    ).astype(jnp.bfloat16)


def clamped_unit(gate_sum, up_sum):
    gate_sum = jnp.minimum(gate_sum, LIMIT)
    up_sum = jnp.clip(up_sum, -LIMIT, LIMIT)
    return ((up_sum + 1.0) * gate_sum * jax.nn.sigmoid(ALPHA * gate_sum)).astype(jnp.bfloat16)


def ring_place(device, n):
    odd = lax.rem(device, 2)
    far = device // 2
    return (1 - odd) * far + odd * (n - 1 - far)


def ring_device(place, n):
    odd = place // (n // 2)
    return 2 * ((1 - odd) * place + odd * (n - 1 - place)) + odd


def expert_phase(
    n, block_rows, total_rows, held, gate_ref, up_ref, down_ref, share_ref, mid_ref, out_ref,
    core_out, core_in, sum_out, sum_in, ring_in, ring_out, kept, last_out, last_in,
    f_send, f_recv, x_send, x_recv, g_send, g_recv, c_send, c_recv,
    cs_send, cs_recv, xs_send, xs_recv, r_send, r_recv, l_send, l_recv,
):
    f32, bf16 = jnp.float32, jnp.bfloat16
    me = lax.axis_index("sp")
    tp = lax.axis_index("tp")
    core = lax.rem(tp, 2)
    side = tp // 2
    place = ring_place(me, n)
    targets = (ring_device(lax.rem(place + 1, n), n), ring_device(lax.rem(place + n - 1, n), n))
    other_core = side * 2 + 1 - core
    other_side = (1 - side) * 2 + core
    half = held.shape[4]
    width = held.shape[5]
    rest = half - total_rows
    block_head, block_tail = pl.ds(0, block_rows), pl.ds(block_rows, half - block_rows)
    total_head, total_tail = pl.ds(0, total_rows), pl.ds(total_rows, rest)
    block_parts = ((0, block_tail), (0, block_head), (1, block_head))
    total_parts = ((0, total_head), (1, total_head), (0, total_tail))

    def owner(h, step):
        return ring_device(lax.rem(place + (n - step if h == 0 else step), n), n)

    def side_of(which):
        return side if which == 0 else 1 - side

    def first_copy(h):
        block = held.at[me, h, core, side, block_head]
        return remote(block, block, f_send.at[h], f_recv.at[h], (me, other_side))

    def first_arrival(h):
        block = held.at[me, h, core, 1 - side, block_head]
        return remote(block, block, f_send.at[h], f_recv.at[h], (me, other_side))

    def side_copy(h, step):
        block = held.at[owner(h, step), h, core, side, block_tail]
        return remote(block, block, x_send.at[h, step], x_recv.at[h, step], (me, other_side))

    def side_arrival(h, step):
        block = held.at[owner(h, step), h, core, 1 - side, block_tail]
        return remote(block, block, x_send.at[h, step], x_recv.at[h, step], (me, other_side))

    def ring_copy(h, step, i):
        which, rows = block_parts[i]
        block = held.at[owner(h, step), h, core, side_of(which), rows]
        return remote(
            block, block, g_send.at[h, i, step], g_recv.at[h, i, step + 1], (targets[h], tp)
        )

    def ring_arrival(h, step, i):
        which, rows = block_parts[i]
        block = held.at[owner(h, step), h, core, side_of(which), rows]
        return remote(block, block, g_send.at[h, i, step], g_recv.at[h, i, step], (targets[h], tp))

    def core_copy(which, h, step):
        block = held.at[owner(h, step), h, core, side_of(which)]
        return remote(
            block, block, c_send.at[which, h, step], c_recv.at[which, h, step], (me, other_core)
        )

    def core_arrival(which, h, step):
        block = held.at[owner(h, step), h, 1 - core, side_of(which)]
        return remote(
            block, block, c_send.at[which, h, step], c_recv.at[which, h, step], (me, other_core)
        )

    def core_sums(which, step):
        return remote(
            core_out.at[step, which], core_in.at[step, which],
            cs_send.at[which, step], cs_recv.at[which, step], (me, other_core),
        )

    def side_sums(h, step):
        return remote(
            sum_out.at[step, h], sum_in.at[step, h],
            xs_send.at[h, step], xs_recv.at[h, step], (me, other_side),
        )

    def total_copy(h, step, i):
        which, rows = total_parts[i]
        later = lax.rem(step + 1, n)
        return remote(
            ring_out.at[step, h, which, rows], ring_in.at[later, h, which, rows],
            r_send.at[h, i, step], r_recv.at[h, i, later], (targets[h], tp),
        )

    def total_arrival(h, step, i):
        which, rows = total_parts[i]
        return remote(
            ring_out.at[step, h, which, rows], ring_in.at[step, h, which, rows],
            r_send.at[h, i, step], r_recv.at[h, i, step], (targets[h], tp),
        )

    def last_copy(h):
        return remote(last_out.at[h], last_in.at[h], l_send.at[h], l_recv.at[h], (me, other_side))

    for h in range(2):
        first_copy(h).start()
    ring_in[1] = jnp.zeros(ring_in.shape[1:], bf16)

    def pass_part(step, i):
        for h in range(2):
            @pl.when(step > 0)
            def _():
                ring_arrival(h, step, i).wait_recv()

            if i == 2:
                @pl.when(step == 0)
                def _():
                    first_arrival(h).wait_recv()

            @pl.when(step < n - 1)
            def _():
                ring_copy(h, step, i).start()

            if i == 1:
                core_copy(0, h, step).start()

    def send_side(step):
        for h in range(2):
            side_copy(h, step).start()

    def share_sides(step):
        for h in range(2):
            side_arrival(h, step).wait_recv()
            core_copy(1, h, step).start()

    def compute(step):
        now = lax.rem(step, kept.shape[0])
        for h in range(2):
            for which in range(2):
                core_arrival(which, h, step).wait_recv()
        owners = (owner(0, step), owner(1, step))
        rows = jnp.concatenate(
            [
                jnp.concatenate([held[owners[h], h, t % 2, t // 2] for t in range(4)], axis=1)
                for h in range(2)
            ],
            axis=0,
        )
        gate_sum = jnp.dot(rows, gate_ref[...], preferred_element_type=f32)
        up_sum = jnp.dot(rows, up_ref[...], preferred_element_type=f32)
        units = clamped_unit(gate_sum, up_sum)
        share = jnp.concatenate(
            [share_ref[owners[h], h * half : (h + 1) * half] for h in range(2)], axis=0
        )
        share = jnp.concatenate([share] * (width // 128), axis=1)

        def part_of(c, which):
            columns = pl.ds(pl.multiple_of((2 * side_of(which) + c) * width, width), width)
            return jnp.dot(units, down_ref[:, columns], preferred_element_type=f32) * share

        for which in (1, 0):
            core_out[step, which] = part_of(1 - core, which).astype(bf16)
            core_sums(which, step).start()
        for which in (1, 0):
            kept[now, which] = part_of(core, which)

    def total_part(step, i):
        now = lax.rem(step, kept.shape[0])
        which, rows = total_parts[i]
        for h in range(2):
            start = h * half + rows.start
            value = kept[now, which, start : start + rows.size]
            if i == 2:
                side_sums(h, step).wait_recv()
                value = value + sum_in[step, h].astype(f32)

            @pl.when(step > 1)
            def _():
                total_arrival(h, step, i).wait_recv()

            ring_out[step, h, which, rows] = (
                value + ring_in[step, h, which, rows].astype(f32)
            ).astype(bf16)
            total_copy(h, step, i).start()

    def pair_sums(step):
        now = lax.rem(step, kept.shape[0])
        for which in (1, 0):
            core_sums(which, step).wait_recv()
            value = kept[now, which] + core_in[step, which].astype(f32)
            if which == 1:
                for h in range(2):
                    sum_out[step, h] = value[h * half + total_rows : (h + 1) * half].astype(bf16)
                    side_sums(h, step).start()
            kept[now, which] = value

    order = (
        (lambda step: pass_part(step, 0), 0, 0, n - 1),
        (send_side, 0, 0, n - 1),
        (lambda step: total_part(step, 0), 5, 1, n - 1),
        (lambda step: pair_sums(lax.rem(step, n)), 3, 1, n),
        (lambda step: total_part(step, 1), 3, 1, n - 1),
        (lambda step: pass_part(step, 1), 0, 0, n - 1),
        (lambda step: compute(lax.rem(step, n)), 2, 1, n),
        (lambda step: pass_part(step, 2), 1, 0, n - 1),
        (share_sides, 1, 0, n - 1),
        (lambda step: total_part(step, 2), 4, 1, n - 1),
    )

    def one_step(i, carry):
        for run, lag, low, high in order:
            pl.when((i >= low + lag) & (i <= high + lag))(functools.partial(run, i - lag))
        return carry

    lax.fori_loop(0, n + 5, one_step, 0)
    for h in range(2):
        rows = pl.ds(h * half, total_rows)
        total_arrival(h, 0, 1).wait_recv()
        last_out[h] = (kept[0, 1, rows] + ring_in[0, h, 1, total_head].astype(f32)).astype(bf16)
        last_copy(h).start()
    for h in range(2):
        rows = pl.ds(h * half + total_rows, rest)
        total_arrival(h, 0, 2).wait_recv()
        side_sums(h, 0).wait_recv()
        value = kept[0, 0, rows] + ring_in[0, h, 0, total_tail].astype(f32) + sum_in[0, h].astype(f32)
        out_ref[rows, :] = (mid_ref[rows, :].astype(f32) + value).astype(bf16)
    for h in range(2):
        rows = pl.ds(h * half, total_rows)
        total_arrival(h, 0, 0).wait_recv()
        last_copy(h).wait_recv()
        value = kept[0, 0, rows] + ring_in[0, h, 0, total_head].astype(f32) + last_in[h].astype(f32)
        out_ref[rows, :] = (mid_ref[rows, :].astype(f32) + value).astype(bf16)
        first_copy(h).wait_send()
        last_copy(h).wait_send()

    def finish(step, carry):
        for h in range(2):
            side_copy(h, step).wait_send()
            side_sums(h, step).wait_send()
            core_sums(h, step).wait_send()
            for which in range(2):
                core_copy(which, h, step).wait_send()
            for i in range(3):
                @pl.when(step < n - 1)
                def _():
                    ring_copy(h, step, i).wait_send()

                @pl.when(step > 0)
                def _():
                    total_copy(h, step, i).wait_send()

        return carry

    lax.fori_loop(0, n, finish, 0)


def flip(z, k, bits):
    out = 0
    for b in range(bits):
        zb = (z // (1 << b)) % 2
        kb = (k // (1 << b)) % 2
        out = out + (zb + kb - 2 * zb * kb) * (1 << b)
    return out


def remote(src, dst, send, recv, peer):
    return pltpu.make_async_remote_copy(
        src_ref=src, dst_ref=dst, send_sem=send, recv_sem=recv,
        device_id=peer, device_id_type=pl.DeviceIdType.MESH,
    )


def lanes_to_rows(row):
    return jnp.transpose(jnp.broadcast_to(row, (128, row.shape[1])))


def layer_kernel(
    n, head, block_rows, total_rows, q_ref, kt_ref, vt_ref, qg_ref, kg_ref, ag_ref, fg_ref, rt_ref,
    rw_ref, cos_hbm, sin_hbm, res_hbm, w_hbm, gate_hbm, up_hbm, down_hbm, out_ref,
    cos_ref, sin_ref, res_ref, w_ref,
    gate_ref, up_ref, down_ref, held, mid_ref, share_ref, w_sem,
    kv_all, q_all, m_s, l_s, acc, att_all, ss_all, sh_own, sh_all,
    z_send, kv_recv, y_send, sh_send, sh_recv, a_send, a_recv, s_send, s_recv,
    *expert_refs,
):
    f32, bf16 = jnp.float32, jnp.bfloat16
    me = lax.axis_index("sp")
    tp = lax.axis_index("tp")
    core = tp % 2
    side = tp // 2
    other_core = side * 2 + 1 - core
    other_side = (1 - side) * 2 + core
    corner = (1 - side) * 2 + 1 - core
    nz = n // 2
    bits = nz.bit_length() - 1
    z = me // 2
    y = me % 2
    pair = 2 * z + 1 - y
    tokens = q_ref.shape[0]
    heads = q_ref.shape[1] // head
    quarter = head // 2

    barrier = pltpu.get_barrier_semaphore()
    for d in range(1, n):
        pl.semaphore_signal(
            barrier, inc=1, device_id=((me + d) % n, tp), device_id_type=pl.DeviceIdType.MESH
        )
    for peer in (other_core, other_side, corner):
        pl.semaphore_signal(
            barrier, inc=1, device_id=(me, peer), device_id_type=pl.DeviceIdType.MESH
        )

    sources = (
        cos_hbm.at[me], sin_hbm.at[me], w_hbm, res_hbm, gate_hbm.at[0], up_hbm.at[0], down_hbm.at[0]
    )
    landings = (cos_ref, sin_ref, w_ref, res_ref, gate_ref, up_ref, down_ref)
    loads = [
        pltpu.make_async_copy(src, dst, w_sem.at[i])
        for i, (src, dst) in enumerate(zip(sources, landings))
    ]
    for load in loads:
        load.start()
    loads[0].wait()
    loads[1].wait()
    cos_t = cos_ref[...]
    sin_t = sin_ref[...]
    key = kt_ref[...].astype(f32)
    gain_rows = lanes_to_rows(jnp.concatenate([kg_ref[...], kg_ref[...]], axis=1))[:head, :1]
    mean = jnp.sum(key * key, axis=0, keepdims=True) / head
    scaled = key * lax.rsqrt(mean + EPS) * gain_rows
    first, second = scaled[:quarter], scaled[quarter:]
    kv_all[me, :quarter, :] = (first * cos_t - second * sin_t).astype(bf16)
    kv_all[me, quarter:head, :] = (first * sin_t + second * cos_t).astype(bf16)
    kv_all[me, head:, :] = vt_ref[...]

    cos_q = jnp.transpose(jnp.concatenate([cos_t] * 4, axis=0))
    sin_q = jnp.transpose(jnp.concatenate([-sin_t, sin_t] * 2, axis=0))
    lane = lax.broadcasted_iota(jnp.int32, (tokens, 128), 1)
    low = lane < head
    near = lane % head < quarter
    gain_q = jnp.concatenate([qg_ref[...], qg_ref[...]], axis=1)
    for j in range(heads // 2):
        x = q_ref[:, 128 * j : 128 * (j + 1)].astype(f32)
        square = x * x
        even = jnp.sum(jnp.where(low, square, 0.0), axis=1, keepdims=True)
        odd = jnp.sum(jnp.where(low, 0.0, square), axis=1, keepdims=True)
        inverse = lax.rsqrt(jnp.where(low, even, odd) / head + EPS)
        scaled = x * inverse * gain_q
        partner = jnp.where(
            near, pltpu.roll(scaled, 128 - quarter, 1), pltpu.roll(scaled, quarter, 1)
        )
        turned = (scaled * cos_q + partner * sin_q).astype(bf16).astype(f32) * (head**-0.5)
        q_all[2 * j] = jnp.where(low, turned, 0.0).astype(bf16)
        q_all[2 * j + 1] = jnp.where(low, 0.0, turned).astype(bf16)

    m_s[...] = jnp.full(m_s.shape, -1e30, f32)
    l_s[...] = jnp.zeros(l_s.shape, f32)
    acc[...] = jnp.zeros(acc.shape, f32)

    pl.semaphore_wait(barrier, n + 2)

    def partner(k):
        return flip(z, (nz - k) % nz, bits)

    def z_copy(k):
        return remote(
            kv_all.at[me], kv_all.at[me], z_send.at[k], kv_recv.at[me],
            (2 * partner(k) + y, tp),
        )

    def y_copy(k):
        block = 2 * partner(k) + y
        return remote(
            kv_all.at[block], kv_all.at[block], y_send.at[k], kv_recv.at[block], (pair, tp)
        )

    def arrival(block):
        return remote(kv_all.at[block], kv_all.at[block], z_send.at[0], kv_recv.at[block], (pair, tp))

    y_copy(0).start()
    for k in range(1, nz):
        z_copy(k).start()

    chosen = jnp.zeros((sh_all.shape[0], tokens), f32)
    expert = lax.broadcasted_iota(jnp.int32, chosen.shape, 0)
    for k in range(rt_ref.shape[0]):
        chosen = chosen + jnp.where(expert == rt_ref[k : k + 1, :], rw_ref[k : k + 1, :], 0.0)
    for e in range(n):
        sh_own[e] = chosen[e : e + 1, :]

    def share_copy(d):
        to = (me + d) % n
        return remote(sh_own.at[to], sh_all.at[me], sh_send.at[d], sh_recv.at[me], (to, tp))

    def share_arrival(d):
        block = (me + n - d) % n
        return remote(sh_own.at[me], sh_all.at[block], sh_send.at[d], sh_recv.at[block], (block, tp))

    for d in range(1, n):
        share_copy(d).start()
    sh_all[me] = sh_own[me]

    def group_step(k, carry):
        @pl.when(k < nz - 1)
        def _():
            arrival(2 * partner(k + 1) + y).wait_recv()
            y_copy(k + 1).start()

        other = 2 * partner(k) + 1 - y
        arrival(other).wait_recv()
        both = jnp.concatenate([kv_all[2 * partner(k) + y], kv_all[other]], axis=1)
        kk = jnp.concatenate([both[:head], both[:head]], axis=0)
        vv = jnp.concatenate([both[head:], both[head:]], axis=0)
        pieces = both.shape[1] // 128
        for h in range(heads):
            scores = jnp.dot(q_all[h], kk, preferred_element_type=f32)
            old = m_s[h]
            new = jnp.maximum(old, jnp.max(scores, axis=1, keepdims=True))
            weights = jnp.exp(scores - jnp.concatenate([new] * pieces, axis=1))
            factor = jnp.exp(old - new)
            part = weights[:, :128]
            for i in range(1, pieces):
                part = part + weights[:, 128 * i : 128 * (i + 1)]
            l_s[h] = l_s[h] * factor + part
            acc[h] = acc[h] * factor + lax.dot_general(
                weights.astype(bf16), vv, (((1,), (1,)), ((), ())), preferred_element_type=f32
            )
            m_s[h] = new
        return carry

    lax.fori_loop(0, nz, group_step, 0)

    for j in range(heads // 2):
        even = acc[2 * j] / jnp.sum(l_s[2 * j], axis=1, keepdims=True)
        odd = acc[2 * j + 1] / jnp.sum(l_s[2 * j + 1], axis=1, keepdims=True)
        att_all[tp, :, 128 * j : 128 * (j + 1)] = jnp.where(low, even, odd).astype(bf16)

    def head_copy(i, slot, peer):
        return remote(att_all.at[slot], att_all.at[slot], a_send.at[i], a_recv.at[slot], (me, peer))

    head_copies = (
        head_copy(0, tp, other_side), head_copy(1, tp, other_core), head_copy(2, other_side, other_core)
    )
    head_copies[0].start()
    head_copies[1].start()
    for d in range(1, n):
        share_arrival(d).wait_recv()
    for b in range(n):
        share_ref[b] = lanes_to_rows(sh_all[b])
    head_copy(0, other_side, other_side).wait_recv()
    head_copies[2].start()
    head_copy(1, other_core, other_core).wait_recv()
    head_copy(2, corner, other_core).wait_recv()

    loads[2].wait()
    loads[3].wait()
    every = jnp.concatenate([att_all[t] for t in range(4)], axis=1).astype(f32)
    mean = jnp.mean(every * every, axis=1, keepdims=True)
    normed = (every * lax.rsqrt(mean + EPS) * ag_ref[...]).astype(bf16)
    mid = (
        res_ref[...].astype(f32) + jnp.dot(normed, w_ref[...], preferred_element_type=f32)
    ).astype(bf16)
    mid_ref[...] = mid
    mid_f = mid.astype(f32)
    square = mid_f * mid_f
    width = mid.shape[1]
    part = square[:, :128]
    for i in range(1, width // 128):
        part = part + square[:, 128 * i : 128 * (i + 1)]
    own = jnp.sum(jnp.transpose(part), axis=0, keepdims=True)
    ss_all[tp] = jnp.broadcast_to(own, ss_all.shape[1:])

    def sum_copy(i, slot, peer):
        return remote(ss_all.at[slot], ss_all.at[slot], s_send.at[i], s_recv.at[slot], (me, peer))

    peers = (other_side, corner, other_core)
    for i, peer in enumerate(peers):
        sum_copy(i, tp, peer).start()
    for i, peer in enumerate(peers):
        sum_copy(i, peer, peer).wait_recv()
    total = (ss_all[0] + ss_all[1]) + (ss_all[2] + ss_all[3])
    inverse = lax.rsqrt(lanes_to_rows(total[:1]) / (4 * width) + EPS)
    ffn_in = (
        mid_f * jnp.concatenate([inverse] * (width // 128), axis=1) * fg_ref[...]
    ).astype(bf16)
    half = tokens // 2
    for h in range(2):
        held[me, h, core, side] = ffn_in[h * half : (h + 1) * half]
    for load in loads[4:]:
        load.wait()
    expert_phase(
        n, block_rows, total_rows, held, gate_ref, up_ref, down_ref, share_ref, mid_ref, out_ref, *expert_refs
    )

    for k in range(nz):
        y_copy(k).wait_send()
    for k in range(1, nz):
        z_copy(k).wait_send()
    for d in range(1, n):
        share_copy(d).wait_send()
    for copy in head_copies:
        copy.wait_send()
    for i, peer in enumerate(peers):
        sum_copy(i, tp, peer).wait_send()


def whole_layer(args, n, head):
    (queries, keys, values, query_gain, key_norm_gain, attn_gain, residual, out_weight, ffn_gain,
     routes, route_weight, gate_weight, up_weight, down_weight) = args
    tokens, width = residual.shape
    full, hidden = gate_weight.shape[1:]
    half = tokens // 2
    block_rows, total_rows = BLOCK_ROWS * half // 8, TOTAL_ROWS * half // 8
    rest = half - total_rows
    hbm = pl.BlockSpec(memory_space=pl.ANY)
    heads = queries.shape[1] // head
    f32, bf16 = jnp.float32, jnp.bfloat16
    dma = pltpu.SemaphoreType.DMA
    vmem = pl.BlockSpec(memory_space=pltpu.VMEM)
    positions = np.arange(n * tokens)
    steps = np.float32(THETA) ** (-np.arange(0, head // 2, 2, dtype=np.float32) / np.float32(head // 2))
    angles = np.concatenate(
        [
            (positions // GRID_W).astype(np.float32)[:, None] * steps,
            (positions % GRID_W).astype(np.float32)[:, None] * steps,
        ],
        axis=1,
    ).reshape(n, tokens, head // 2).transpose(0, 2, 1)
    rows = max(8, n)
    return pl.pallas_call(
        functools.partial(layer_kernel, n, head, block_rows, total_rows),
        out_shape=jax.ShapeDtypeStruct((tokens, width), bf16),
        in_specs=[vmem] * 9 + [hbm] * 7,
        out_specs=vmem,
        scratch_shapes=[
            pltpu.VMEM((head // 2, tokens), f32),
            pltpu.VMEM((head // 2, tokens), f32),
            pltpu.VMEM((tokens, width), bf16),
            pltpu.VMEM(out_weight.shape, bf16),
            pltpu.VMEM((full, hidden), bf16),
            pltpu.VMEM((full, hidden), bf16),
            pltpu.VMEM((hidden, full), bf16),
            pltpu.VMEM((n, 2, 2, 2, half, width), bf16),
            pltpu.VMEM((tokens, width), bf16),
            pltpu.VMEM((n, tokens, 128), f32),
            dma((7,)),
            pltpu.VMEM((n, 2 * head, tokens), bf16),
            pltpu.VMEM((heads, tokens, 128), bf16),
            pltpu.VMEM((heads, tokens, 128), f32),
            pltpu.VMEM((heads, tokens, 128), f32),
            pltpu.VMEM((heads, tokens, 128), f32),
            pltpu.VMEM((4, tokens, heads * head), bf16),
            pltpu.VMEM((4, 8, tokens), f32),
            pltpu.VMEM((rows, 1, tokens), f32),
            pltpu.VMEM((rows, 1, tokens), f32),
            dma((n // 2,)), dma((n,)), dma((n // 2,)), dma((n,)), dma((n,)),
            dma((3,)), dma((4,)), dma((3,)), dma((4,)),
            pltpu.VMEM((n, 2, tokens, width), bf16),
            pltpu.VMEM((n, 2, tokens, width), bf16),
            pltpu.VMEM((n, 2, rest, width), bf16),
            pltpu.VMEM((n, 2, rest, width), bf16),
            pltpu.VMEM((n, 2, 2, half, width), bf16),
            pltpu.VMEM((n, 2, 2, half, width), bf16),
            pltpu.VMEM((4, 2, tokens, width), f32),
            pltpu.VMEM((2, total_rows, width), bf16),
            pltpu.VMEM((2, total_rows, width), bf16),
            dma((2,)), dma((2,)), dma((2, n)), dma((2, n)),
            dma((2, 3, n)), dma((2, 3, n)), dma((2, 2, n)), dma((2, 2, n)),
            dma((2, n)), dma((2, n)), dma((2, n)), dma((2, n)),
            dma((2, 3, n)), dma((2, 3, n)), dma((2,)), dma((2,)),
        ],
        compiler_params=pltpu.CompilerParams(
            collective_id=0, has_side_effects=True, vmem_limit_bytes=60 * 1024 * 1024
        ),
    )(
        queries, keys.T, values.T, query_gain.reshape(1, head), key_norm_gain.reshape(1, head),
        attn_gain.reshape(1, -1), ffn_gain.reshape(1, -1),
        routes.T, route_weight.T,
        np.cos(angles).astype(np.float32), np.sin(angles).astype(np.float32), residual, out_weight,
        gate_weight, up_weight, down_weight,
    )


def per_device(
    queries,
    keys,
    values,
    query_gain,
    key_norm_gain,
    attn_gain,
    residual,
    out_weight,
    ffn_gain,
    routes,
    route_weight,
    gate_weight,
    up_weight,
    down_weight,
):
    tokens = queries.shape[0]
    head_size = query_gain.shape[0]
    experts = lax.axis_size("sp")
    paired = experts >= 4 and experts & (experts - 1) == 0 and experts <= 2 * routes.shape[1]
    if paired and lax.axis_size("tp") == 4 and keys.shape[1] == head_size == 64:
        return whole_layer(
            (queries, keys, values, query_gain, key_norm_gain, attn_gain, residual, out_weight,
             ffn_gain, routes, route_weight, gate_weight, up_weight, down_weight),
            experts, head_size,
        )
    kv_local = keys.shape[1] // head_size
    q_local = queries.shape[1] // head_size
    group_width = q_local // kv_local
    first_token = lax.axis_index("sp") * tokens
    positions = first_token + jnp.arange(tokens, dtype=jnp.int32)
    cosine_lookup, sine_lookup = rotary_tables(positions, head_size, GRID_W)
    query_rotated = normalize_then_rotate(
        queries.reshape(tokens, q_local, head_size), query_gain, cosine_lookup, sine_lookup
    )
    key_rotated = normalize_then_rotate(
        keys.reshape(tokens, kv_local, head_size), key_norm_gain, cosine_lookup, sine_lookup
    )
    query_rows = query_rotated.reshape(tokens, kv_local, group_width, head_size).transpose(
        1, 0, 2, 3
    )
    query_rows = query_rows.reshape(kv_local, tokens * group_width, head_size)
    value_rows = values.reshape(tokens, kv_local, head_size)
    score_scale = head_size ** (-0.5)
    query_width = tokens * group_width
    start_state = (
        jnp.full((kv_local, query_width), -1e30, jnp.float32),
        jnp.zeros((kv_local, query_width), jnp.float32),
        jnp.zeros((kv_local, query_width, head_size), jnp.float32),
    )
    kv_width = kv_local * head_size
    packed = jnp.concatenate([key_rotated.reshape(tokens, kv_width), values], axis=1)
    gathered = lax.all_gather(packed, "sp", axis=0, tiled=True)
    piece_keys = gathered[:, :kv_width].reshape(-1, kv_local, head_size)
    piece_values = gathered[:, kv_width:].reshape(-1, kv_local, head_size)
    slot_count = piece_keys.shape[0]
    block_rows = 2048
    key_blocks = piece_keys.reshape(slot_count // block_rows, block_rows, kv_local, head_size)
    value_blocks = piece_values.reshape(slot_count // block_rows, block_rows, kv_local, head_size)

    def one_block(softmax_state, pair_block):
        running_max, running_sum, accumulated = softmax_state
        key_block, value_block = pair_block
        scores = (
            jnp.einsum("kqd,nkd->kqn", query_rows, key_block, preferred_element_type=jnp.float32)
            * score_scale
        )
        new_max = jnp.maximum(running_max, jnp.max(scores, axis=-1))
        weights = jnp.exp(scores - new_max[..., None])
        factor = jnp.exp(running_max - new_max)
        running_sum = running_sum * factor + jnp.sum(weights, axis=-1)
        accumulated = accumulated * factor[..., None] + jnp.einsum(
            "kqn,nkd->kqd",
            weights.astype(jnp.bfloat16),
            value_block,
            preferred_element_type=jnp.float32,
        )
        return ((new_max, running_sum, accumulated), None)

    final_state, unused_out = lax.scan(one_block, start_state, (key_blocks, value_blocks))
    running_max, running_sum, accumulated = final_state
    attended = (accumulated / running_sum[..., None]).reshape(
        kv_local, tokens, group_width, head_size
    )
    attended = (
        attended.transpose(1, 0, 2, 3).reshape(tokens, q_local * head_size).astype(jnp.bfloat16)
    )
    all_heads = lax.all_gather(attended, "tp", axis=1, tiled=True)
    head_f = all_heads.astype(jnp.float32)
    attn_normed = (
        head_f * lax.rsqrt(jnp.mean(head_f * head_f, axis=-1, keepdims=True) + EPS) * attn_gain
    ).astype(jnp.bfloat16)
    mid_stream = (
        residual.astype(jnp.float32)
        + jnp.dot(attn_normed, out_weight, preferred_element_type=jnp.float32)
    ).astype(jnp.bfloat16)
    mid_f = mid_stream.astype(jnp.float32)
    square_total = lax.psum(jnp.sum(mid_f * mid_f, axis=-1), "tp")
    ffn_in = (mid_f * lax.rsqrt(square_total / D + EPS)[:, None] * ffn_gain).astype(jnp.bfloat16)
    top_k = routes.shape[1]
    capacity = tokens * top_k * 3 // (2 * experts)
    route_list = routes.reshape(-1)
    onehot = (route_list[:, None] == jnp.arange(experts, dtype=jnp.int32)[None, :]).astype(
        jnp.int32
    )
    route_ranks = jnp.sum((jnp.cumsum(onehot, axis=0) - 1) * onehot, axis=1)
    slot_index = route_list * capacity + route_ranks
    slot_owner = (
        jnp.full((experts * capacity,), tokens, jnp.int32)
        .at[slot_index]
        .set(jnp.arange(tokens * top_k, dtype=jnp.int32) // top_k)
    )
    padded = jnp.concatenate([ffn_in, jnp.zeros((1, ffn_in.shape[1]), ffn_in.dtype)], axis=0)
    slot_block = lax.all_to_all(
        padded[slot_owner].reshape(experts, capacity, ffn_in.shape[1]),
        "sp",
        split_axis=0,
        concat_axis=0,
        tiled=True,
    )
    slot_count = slot_block.shape[1]
    slot_rows = slot_block.reshape(-1, slot_block.shape[2])
    column_piece = lax.all_gather(slot_rows, "tp", axis=1, tiled=True)
    gate_rows = gate_weight[0]
    up_rows = up_weight[0]
    gate_sum = jnp.dot(column_piece, gate_rows, preferred_element_type=jnp.float32)
    up_sum = jnp.dot(column_piece, up_rows, preferred_element_type=jnp.float32)
    partial_value = jnp.dot(
        clamped_unit(gate_sum, up_sum), down_weight[0], preferred_element_type=jnp.float32
    )
    summed = lax.psum_scatter(
        partial_value.astype(jnp.bfloat16), "tp", scatter_dimension=1, tiled=True
    )
    results = lax.all_to_all(
        summed.reshape(experts, slot_count, summed.shape[1]),
        "sp",
        split_axis=0,
        concat_axis=0,
        tiled=True,
    )
    picked = results.reshape(experts * capacity, -1)[slot_index].astype(jnp.float32)
    weighted = jnp.sum(
        (picked * route_weight.reshape(-1)[:, None]).reshape(tokens, top_k, -1), axis=1
    )
    return (mid_f + weighted).astype(jnp.bfloat16)


def solution(mesh):
    placed = (
        P("sp", "tp"),
        P("sp", "tp"),
        P("sp", "tp"),
        P(),
        P(),
        P(),
        P("sp", "tp"),
        P(None, "tp"),
        P("tp"),
        P("sp", None),
        P("sp", None),
        P("sp", None, "tp"),
        P("sp", None, "tp"),
        P("sp", "tp", None),
    )
    return jax.shard_map(
        per_device, mesh=mesh, in_specs=placed, out_specs=P("sp", "tp"), check_vma=False
    )
```

```python
import functools

import jax
import jax.numpy as jnp
import numpy as np
from jax import lax
from jax.experimental import pallas as pl
from jax.experimental.pallas import tpu as pltpu
from jax.sharding import PartitionSpec as P

D = 2048
GRID_W = 64


EPS = 1e-06
THETA = 10000.0
ALPHA = 1.702
LIMIT = 7.0
BLOCK_ROWS = 4
TOTAL_ROWS = 3


def rotary_tables(positions, head_size, grid_width):
    row_pos = (positions // grid_width).astype(jnp.float32)
    col_pos = (positions % grid_width).astype(jnp.float32)
    half_size = head_size // 2
    inverse = THETA ** (-jnp.arange(0, half_size, 2, dtype=jnp.float32) / half_size)
    angles = jnp.concatenate([row_pos[:, None] * inverse, col_pos[:, None] * inverse], axis=-1)
    return (jnp.cos(angles), jnp.sin(angles))


def normalize_then_rotate(head_rows, gain_vector, cosine_lookup, sine_lookup):
    values_f = head_rows.astype(jnp.float32)
    scaled = (
        values_f
        * lax.rsqrt(jnp.mean(values_f * values_f, axis=-1, keepdims=True) + EPS)
        * gain_vector
    )
    first_half, second_half = jnp.split(scaled, 2, axis=-1)
    cos_part = cosine_lookup[:, None, :]
    sin_part = sine_lookup[:, None, :]
    return jnp.concatenate(
        [
            first_half * cos_part - second_half * sin_part,
            first_half * sin_part + second_half * cos_part,
        ],
        axis=-1,
    ).astype(jnp.bfloat16)


def clamped_unit(gate_sum, up_sum):
    gate_sum = jnp.minimum(gate_sum, LIMIT)
    up_sum = jnp.clip(up_sum, -LIMIT, LIMIT)
    return ((up_sum + 1.0) * gate_sum * jax.nn.sigmoid(ALPHA * gate_sum)).astype(jnp.bfloat16)


def ring_place(device, n):
    odd = lax.rem(device, 2)
    far = device // 2
    return (1 - odd) * far + odd * (n - 1 - far)


def ring_device(place, n):
    odd = place // (n // 2)
    return 2 * ((1 - odd) * place + odd * (n - 1 - place)) + odd


def expert_phase(
    n, block_rows, total_rows, held, gate_ref, up_ref, down_ref, share_ref, inv_ref, gain_all, settle, gather_norms, mid_ref, out_ref,
    core_out, core_in, sum_out, sum_in, ring_in, ring_out, kept, last_out, last_in,
    f_send, f_recv, x_send, x_recv, g_send, g_recv, c_send, c_recv,
    cs_send, cs_recv, xs_send, xs_recv, r_send, r_recv, l_send, l_recv,
):
    f32, bf16 = jnp.float32, jnp.bfloat16
    me = lax.axis_index("sp")
    tp = lax.axis_index("tp")
    core = lax.rem(tp, 2)
    side = tp // 2
    place = ring_place(me, n)
    targets = (ring_device(lax.rem(place + 1, n), n), ring_device(lax.rem(place + n - 1, n), n))
    other_core = side * 2 + 1 - core
    other_side = (1 - side) * 2 + core
    half = held.shape[4]
    width = held.shape[5]
    rest = half - total_rows
    block_head, block_tail = pl.ds(0, block_rows), pl.ds(block_rows, half - block_rows)
    total_head, total_tail = pl.ds(0, total_rows), pl.ds(total_rows, rest)
    block_parts = ((0, block_tail), (0, block_head), (1, block_head))
    total_parts = ((0, total_head), (1, total_head), (0, total_tail))

    def owner(h, step):
        return ring_device(lax.rem(place + (n - step if h == 0 else step), n), n)

    def side_of(which):
        return side if which == 0 else 1 - side

    def first_copy(h):
        block = held.at[me, h, core, side, block_head]
        return remote(block, block, f_send.at[h], f_recv.at[h], (me, other_side))

    def first_arrival(h):
        block = held.at[me, h, core, 1 - side, block_head]
        return remote(block, block, f_send.at[h], f_recv.at[h], (me, other_side))

    def side_copy(h, step):
        block = held.at[owner(h, step), h, core, side, block_tail]
        return remote(block, block, x_send.at[h, step], x_recv.at[h, step], (me, other_side))

    def side_arrival(h, step):
        block = held.at[owner(h, step), h, core, 1 - side, block_tail]
        return remote(block, block, x_send.at[h, step], x_recv.at[h, step], (me, other_side))

    def ring_copy(h, step, i):
        which, rows = block_parts[i]
        block = held.at[owner(h, step), h, core, side_of(which), rows]
        return remote(
            block, block, g_send.at[h, i, step], g_recv.at[h, i, step + 1], (targets[h], tp)
        )

    def ring_arrival(h, step, i):
        which, rows = block_parts[i]
        block = held.at[owner(h, step), h, core, side_of(which), rows]
        return remote(block, block, g_send.at[h, i, step], g_recv.at[h, i, step], (targets[h], tp))

    def core_copy(which, h, step):
        block = held.at[owner(h, step), h, core, side_of(which)]
        return remote(
            block, block, c_send.at[which, h, step], c_recv.at[which, h, step], (me, other_core)
        )

    def core_arrival(which, h, step):
        block = held.at[owner(h, step), h, 1 - core, side_of(which)]
        return remote(
            block, block, c_send.at[which, h, step], c_recv.at[which, h, step], (me, other_core)
        )

    def core_sums(which, step):
        return remote(
            core_out.at[step, which], core_in.at[step, which],
            cs_send.at[which, step], cs_recv.at[which, step], (me, other_core),
        )

    def side_sums(h, step):
        return remote(
            sum_out.at[step, h], sum_in.at[step, h],
            xs_send.at[h, step], xs_recv.at[h, step], (me, other_side),
        )

    def total_copy(h, step, i):
        which, rows = total_parts[i]
        later = lax.rem(step + 1, n)
        return remote(
            ring_out.at[step, h, which, rows], ring_in.at[later, h, which, rows],
            r_send.at[h, i, step], r_recv.at[h, i, later], (targets[h], tp),
        )

    def total_arrival(h, step, i):
        which, rows = total_parts[i]
        return remote(
            ring_out.at[step, h, which, rows], ring_in.at[step, h, which, rows],
            r_send.at[h, i, step], r_recv.at[h, i, step], (targets[h], tp),
        )

    def last_copy(h):
        return remote(last_out.at[h], last_in.at[h], l_send.at[h], l_recv.at[h], (me, other_side))

    for h in range(2):
        first_copy(h).start()
    ring_in[1] = jnp.zeros(ring_in.shape[1:], bf16)

    def pass_part(step, i):
        for h in range(2):
            @pl.when(step > 0)
            def _():
                ring_arrival(h, step, i).wait_recv()

            if i == 2:
                @pl.when(step == 0)
                def _():
                    first_arrival(h).wait_recv()

            @pl.when(step < n - 1)
            def _():
                ring_copy(h, step, i).start()

            if i == 1:
                core_copy(0, h, step).start()

    def send_side(step):
        for h in range(2):
            side_copy(h, step).start()

    def share_sides(step):
        for h in range(2):
            side_arrival(h, step).wait_recv()
            core_copy(1, h, step).start()

    def normed_rows(block, h, t):
        inverse = inv_ref[block, h * half : (h + 1) * half]
        inverse = jnp.concatenate([inverse] * (width // 128), axis=1)
        return (held[block, h, t % 2, t // 2].astype(f32) * inverse * gain_all[t]).astype(bf16)

    def compute(step):
        now = lax.rem(step, kept.shape[0])
        for h in range(2):
            for which in range(2):
                core_arrival(which, h, step).wait_recv()
        owners = (owner(0, step), owner(1, step))
        rows = jnp.concatenate(
            [
                jnp.concatenate([normed_rows(owners[h], h, t) for t in range(4)], axis=1)
                for h in range(2)
            ],
            axis=0,
        )
        gate_sum = jnp.dot(rows, gate_ref[...], preferred_element_type=f32)
        up_sum = jnp.dot(rows, up_ref[...], preferred_element_type=f32)
        units = clamped_unit(gate_sum, up_sum)
        share = jnp.concatenate(
            [share_ref[owners[h], h * half : (h + 1) * half] for h in range(2)], axis=0
        )
        share = jnp.concatenate([share] * (width // 128), axis=1)

        def part_of(c, which):
            columns = pl.ds(pl.multiple_of((2 * side_of(which) + c) * width, width), width)
            return jnp.dot(units, down_ref[:, columns], preferred_element_type=f32) * share

        for which in (1, 0):
            core_out[step, which] = part_of(1 - core, which).astype(bf16)
            core_sums(which, step).start()
        for which in (1, 0):
            kept[now, which] = part_of(core, which)

    def total_part(step, i):
        now = lax.rem(step, kept.shape[0])
        which, rows = total_parts[i]
        for h in range(2):
            start = h * half + rows.start
            value = kept[now, which, start : start + rows.size]
            if i == 2:
                side_sums(h, step).wait_recv()
                value = value + sum_in[step, h].astype(f32)

            @pl.when(step > 1)
            def _():
                total_arrival(h, step, i).wait_recv()

            ring_out[step, h, which, rows] = (
                value + ring_in[step, h, which, rows].astype(f32)
            ).astype(bf16)
            total_copy(h, step, i).start()

    def pair_sums(step):
        now = lax.rem(step, kept.shape[0])
        for which in (1, 0):
            core_sums(which, step).wait_recv()
            value = kept[now, which] + core_in[step, which].astype(f32)
            if which == 1:
                for h in range(2):
                    sum_out[step, h] = value[h * half + total_rows : (h + 1) * half].astype(bf16)
                    side_sums(h, step).start()
            kept[now, which] = value

    order = (
        (lambda step: pass_part(step, 0), 0, 0, n - 1),
        (send_side, 0, 0, n - 1),
        (lambda step: total_part(step, 0), 5, 1, n - 1),
        (lambda step: pair_sums(lax.rem(step, n)), 3, 1, n),
        (lambda step: total_part(step, 1), 3, 1, n - 1),
        (lambda step: pass_part(step, 1), 0, 0, n - 1),
        (lambda step: compute(lax.rem(step, n)), 2, 1, n),
        (lambda step: pass_part(step, 2), 1, 0, n - 1),
        (share_sides, 1, 0, n - 1),
        (lambda step: total_part(step, 2), 4, 1, n - 1),
        (lambda step: settle(), 0, 0, 0),
        (lambda step: gather_norms(), 2, 0, 0),
    )

    def one_step(i, carry):
        for run, lag, low, high in order:
            pl.when((i >= low + lag) & (i <= high + lag))(functools.partial(run, i - lag))
        return carry

    lax.fori_loop(0, n + 5, one_step, 0)
    for h in range(2):
        rows = pl.ds(h * half, total_rows)
        total_arrival(h, 0, 1).wait_recv()
        last_out[h] = (kept[0, 1, rows] + ring_in[0, h, 1, total_head].astype(f32)).astype(bf16)
        last_copy(h).start()
    for h in range(2):
        rows = pl.ds(h * half + total_rows, rest)
        total_arrival(h, 0, 2).wait_recv()
        side_sums(h, 0).wait_recv()
        value = kept[0, 0, rows] + ring_in[0, h, 0, total_tail].astype(f32) + sum_in[0, h].astype(f32)
        out_ref[rows, :] = (mid_ref[rows, :].astype(f32) + value).astype(bf16)
    for h in range(2):
        rows = pl.ds(h * half, total_rows)
        total_arrival(h, 0, 0).wait_recv()
        last_copy(h).wait_recv()
        value = kept[0, 0, rows] + ring_in[0, h, 0, total_head].astype(f32) + last_in[h].astype(f32)
        out_ref[rows, :] = (mid_ref[rows, :].astype(f32) + value).astype(bf16)
        first_copy(h).wait_send()
        last_copy(h).wait_send()

    def finish(step, carry):
        for h in range(2):
            side_copy(h, step).wait_send()
            side_sums(h, step).wait_send()
            core_sums(h, step).wait_send()
            for which in range(2):
                core_copy(which, h, step).wait_send()
            for i in range(3):
                @pl.when(step < n - 1)
                def _():
                    ring_copy(h, step, i).wait_send()

                @pl.when(step > 0)
                def _():
                    total_copy(h, step, i).wait_send()

        return carry

    lax.fori_loop(0, n, finish, 0)


def flip(z, k, bits):
    out = 0
    for b in range(bits):
        zb = (z // (1 << b)) % 2
        kb = (k // (1 << b)) % 2
        out = out + (zb + kb - 2 * zb * kb) * (1 << b)
    return out


def remote(src, dst, send, recv, peer):
    return pltpu.make_async_remote_copy(
        src_ref=src, dst_ref=dst, send_sem=send, recv_sem=recv,
        device_id=peer, device_id_type=pl.DeviceIdType.MESH,
    )


def lanes_to_rows(row):
    return jnp.transpose(jnp.broadcast_to(row, (128, row.shape[1])))


def layer_kernel(
    n, head, block_rows, total_rows, *refs
):
    sources, out_ref, landings, refs = refs[:16], refs[16], refs[17:32], refs[32:]
    layer_body(n, head, block_rows, total_rows, sources, out_ref, landings, *refs)


def layer_body(
    n, head, block_rows, total_rows, sources, out_ref, landings, gain_all, inv_all, inv_ref,
    n_send, n_recv, gs_send, gs_recv,
    held, mid_ref, share_ref, w_sem,
    kv_all, q_all, m_s, l_s, acc, att_all, ss_all, sh_own, sh_all,
    z_send, kv_recv, y_send, sh_send, sh_recv, a_send, a_recv, s_send, s_recv,
    *expert_refs,
):
    (cos_ref, sin_ref, kt_ref, vt_ref, kg_ref, qg_ref, q_ref, rt_ref, rw_ref, ag_ref, w_ref, res_ref,
     gate_ref, up_ref, down_ref) = landings
    f32, bf16 = jnp.float32, jnp.bfloat16
    me = lax.axis_index("sp")
    tp = lax.axis_index("tp")
    core = tp % 2
    side = tp // 2
    other_core = side * 2 + 1 - core
    other_side = (1 - side) * 2 + core
    corner = (1 - side) * 2 + 1 - core
    nz = n // 2
    bits = nz.bit_length() - 1
    z = me // 2
    y = me % 2
    pair = 2 * z + 1 - y
    tokens = q_ref.shape[0]
    heads = q_ref.shape[1] // head
    quarter = head // 2

    barrier = pltpu.get_barrier_semaphore()
    for d in range(1, n):
        pl.semaphore_signal(
            barrier, inc=1, device_id=((me + d) % n, tp), device_id_type=pl.DeviceIdType.MESH
        )
    for peer in (other_core, other_side, corner):
        pl.semaphore_signal(
            barrier, inc=1, device_id=(me, peer), device_id_type=pl.DeviceIdType.MESH
        )

    sources = [src.at[me] for src in sources[:2]] + list(sources[2:13]) + [
        src.at[0] for src in sources[13:]
    ]
    landings = landings[:2] + landings[2:10] + (gain_all.at[tp],) + landings[10:]
    loads = [
        pltpu.make_async_copy(src, dst, w_sem.at[i])
        for i, (src, dst) in enumerate(zip(sources, landings))
    ]
    for load in loads:
        load.start()
    for load in loads[:5]:
        load.wait()
    cos_t = cos_ref[...]
    sin_t = sin_ref[...]
    key = kt_ref[...].astype(f32)
    gain_rows = lanes_to_rows(jnp.concatenate([kg_ref[...], kg_ref[...]], axis=1))[:head, :1]
    mean = jnp.sum(key * key, axis=0, keepdims=True) / head
    scaled = key * lax.rsqrt(mean + EPS) * gain_rows
    first, second = scaled[:quarter], scaled[quarter:]
    kv_all[me, 0, :quarter, :] = (first * cos_t - second * sin_t).astype(bf16)
    kv_all[me, 0, quarter:, :] = (first * sin_t + second * cos_t).astype(bf16)
    kv_all[me, 1] = vt_ref[...]

    for load in loads[5:11]:
        load.wait()
    cos_q = jnp.transpose(jnp.concatenate([cos_t] * 4, axis=0))
    sin_q = jnp.transpose(jnp.concatenate([-sin_t, sin_t] * 2, axis=0))
    lane = lax.broadcasted_iota(jnp.int32, (tokens, 128), 1)
    low = lane < head
    near = lane % head < quarter
    gain_q = jnp.concatenate([qg_ref[...], qg_ref[...]], axis=1)
    for j in range(heads // 2):
        x = q_ref[:, 128 * j : 128 * (j + 1)].astype(f32)
        square = x * x
        even = jnp.sum(jnp.where(low, square, 0.0), axis=1, keepdims=True)
        odd = jnp.sum(jnp.where(low, 0.0, square), axis=1, keepdims=True)
        inverse = lax.rsqrt(jnp.where(low, even, odd) / head + EPS)
        scaled = x * inverse * gain_q
        partner = jnp.where(
            near, pltpu.roll(scaled, 128 - quarter, 1), pltpu.roll(scaled, quarter, 1)
        )
        turned = (scaled * cos_q + partner * sin_q).astype(bf16).astype(f32) * (head**-0.5)
        q_all[2 * j] = jnp.where(low, turned, 0.0).astype(bf16)
        q_all[2 * j + 1] = jnp.where(low, 0.0, turned).astype(bf16)

    m_s[...] = jnp.full(m_s.shape, -1e30, f32)
    l_s[...] = jnp.zeros(l_s.shape, f32)
    acc[...] = jnp.zeros(acc.shape, f32)

    pl.semaphore_wait(barrier, n + 2)

    def partner(k):
        return flip(z, k, bits)

    def z_copy(k, c):
        return remote(
            kv_all.at[me, c], kv_all.at[me, c], z_send.at[k, c], kv_recv.at[me, c],
            (2 * partner(k) + y, tp),
        )

    def y_copy(k, c):
        block = 2 * partner(k) + y
        return remote(
            kv_all.at[block, c], kv_all.at[block, c], y_send.at[k, c], kv_recv.at[block, c], (pair, tp)
        )

    def arrival(block, c):
        return remote(
            kv_all.at[block, c], kv_all.at[block, c], z_send.at[0, c], kv_recv.at[block, c], (pair, tp)
        )

    for c in range(2):
        y_copy(0, c).start()
    for k in range(nz - 1, 0, -1):
        for c in range(2):
            z_copy(k, c).start()
    peers = (other_side, corner, other_core)

    def gain_copy(i, slot, peer):
        return remote(gain_all.at[slot], gain_all.at[slot], gs_send.at[i], gs_recv.at[slot], (me, peer))

    for i, peer in enumerate(peers):
        gain_copy(i, tp, peer).start()

    chosen = jnp.zeros((sh_all.shape[0], tokens), f32)
    expert = lax.broadcasted_iota(jnp.int32, chosen.shape, 0)
    for k in range(rt_ref.shape[0]):
        chosen = chosen + jnp.where(expert == rt_ref[k : k + 1, :], rw_ref[k : k + 1, :], 0.0)
    for e in range(n):
        sh_own[e] = chosen[e : e + 1, :]

    def share_copy(d):
        to = (me + d) % n
        return remote(sh_own.at[to], sh_all.at[me], sh_send.at[d], sh_recv.at[me], (to, tp))

    def share_arrival(d):
        block = (me + n - d) % n
        return remote(sh_own.at[me], sh_all.at[block], sh_send.at[d], sh_recv.at[block], (block, tp))

    for d in range(1, n):
        share_copy(d).start()
    sh_all[me] = sh_own[me]

    def attend(k, which):
        other = 2 * partner(k) + 1 - y
        mine = 2 * partner(k) + y
        keys = jnp.concatenate([kv_all[mine, 0], kv_all[other, 0]], axis=1)
        values = jnp.concatenate([kv_all[mine, 1], kv_all[other, 1]], axis=1)
        kk = jnp.concatenate([keys, keys], axis=0)
        vv = jnp.concatenate([values, values], axis=0)
        pieces = keys.shape[1] // 128
        for h in which:
            scores = jnp.dot(q_all[h], kk, preferred_element_type=f32)
            old = m_s[h]
            new = jnp.maximum(old, jnp.max(scores, axis=1, keepdims=True))
            weights = jnp.exp(scores - jnp.concatenate([new] * pieces, axis=1))
            factor = jnp.exp(old - new)
            part = weights[:, :128]
            for i in range(1, pieces):
                part = part + weights[:, 128 * i : 128 * (i + 1)]
            l_s[h] = l_s[h] * factor + part
            acc[h] = acc[h] * factor + lax.dot_general(
                weights.astype(bf16), vv, (((1,), (1,)), ((), ())), preferred_element_type=f32
            )
            m_s[h] = new

    def group_step(k, carry):
        for c in range(2):
            arrival(2 * partner(k + 1) + y, c).wait_recv()
            y_copy(k + 1, c).start()
        for c in range(2):
            arrival(2 * partner(k) + 1 - y, c).wait_recv()
        attend(k, range(heads))
        return carry

    lax.fori_loop(0, nz - 1, group_step, 0)

    def head_copy(i, j, slot, peer):
        return remote(
            att_all.at[slot, j], att_all.at[slot, j], a_send.at[i, j], a_recv.at[slot, j], (me, peer)
        )

    for c in range(2):
        arrival(2 * partner(nz - 1) + 1 - y, c).wait_recv()
    for j in range(heads // 2):
        attend(nz - 1, (2 * j, 2 * j + 1))
        even = acc[2 * j] / jnp.sum(l_s[2 * j], axis=1, keepdims=True)
        odd = acc[2 * j + 1] / jnp.sum(l_s[2 * j + 1], axis=1, keepdims=True)
        att_all[tp, j] = jnp.where(low, even, odd).astype(bf16)
        head_copy(0, j, tp, other_side).start()
        head_copy(1, j, tp, other_core).start()
    for d in range(1, n):
        share_arrival(d).wait_recv()
    for b in range(n):
        share_ref[b] = lanes_to_rows(sh_all[b])
    for j in range(heads // 2):
        head_copy(0, j, other_side, other_side).wait_recv()
        head_copy(2, j, other_side, other_core).start()
    for j in range(heads // 2):
        head_copy(1, j, other_core, other_core).wait_recv()
        head_copy(2, j, corner, other_core).wait_recv()

    loads[11].wait()
    loads[12].wait()
    every = jnp.concatenate(
        [att_all[t, j] for t in range(4) for j in range(heads // 2)], axis=1
    ).astype(f32)
    mean = jnp.mean(every * every, axis=1, keepdims=True)
    normed = (every * lax.rsqrt(mean + EPS) * ag_ref[...]).astype(bf16)
    mid = (
        res_ref[...].astype(f32) + jnp.dot(normed, w_ref[...], preferred_element_type=f32)
    ).astype(bf16)
    mid_ref[...] = mid
    mid_f = mid.astype(f32)
    square = mid_f * mid_f
    width = mid.shape[1]
    part = square[:, :128]
    for i in range(1, width // 128):
        part = part + square[:, 128 * i : 128 * (i + 1)]
    ss_all[tp] = jnp.sum(jnp.transpose(part), axis=0, keepdims=True)

    def sum_copy(i, slot, peer):
        return remote(ss_all.at[slot], ss_all.at[slot], s_send.at[i], s_recv.at[slot], (me, peer))

    for i, peer in enumerate(peers):
        sum_copy(i, tp, peer).start()
    half = tokens // 2
    for h in range(2):
        held[me, h, core, side] = mid[h * half : (h + 1) * half]

    def norm_copy(d):
        to = (me + d) % n
        return remote(inv_all.at[me], inv_all.at[me], n_send.at[d], n_recv.at[me], (to, tp))

    def norm_arrival(d):
        block = (me + n - d) % n
        return remote(inv_all.at[block], inv_all.at[block], n_send.at[d], n_recv.at[block], (block, tp))

    def settle():
        for i, peer in enumerate(peers):
            sum_copy(i, peer, peer).wait_recv()
        total = (ss_all[0] + ss_all[1]) + (ss_all[2] + ss_all[3])
        inv_all[me] = lax.rsqrt(total / (4 * width) + EPS)
        for d in range(1, n):
            norm_copy(d).start()

    def gather_norms():
        for d in range(1, n):
            norm_arrival(d).wait_recv()
        for i, peer in enumerate(peers):
            gain_copy(i, peer, peer).wait_recv()
        for b in range(n):
            inv_ref[b] = lanes_to_rows(inv_all[b])

    for load in loads[13:]:
        load.wait()
    expert_phase(
        n, block_rows, total_rows, held, gate_ref, up_ref, down_ref, share_ref,
        inv_ref, gain_all, settle, gather_norms, mid_ref, out_ref, *expert_refs
    )

    for c in range(2):
        for k in range(nz):
            y_copy(k, c).wait_send()
        for k in range(1, nz):
            z_copy(k, c).wait_send()
    for d in range(1, n):
        share_copy(d).wait_send()
    for j in range(heads // 2):
        head_copy(0, j, tp, other_side).wait_send()
        head_copy(1, j, tp, other_core).wait_send()
        head_copy(2, j, other_side, other_core).wait_send()
    for d in range(1, n):
        norm_copy(d).wait_send()
    for i, peer in enumerate(peers):
        sum_copy(i, tp, peer).wait_send()
        gain_copy(i, tp, peer).wait_send()


def whole_layer(args, n, head):
    (queries, keys, values, query_gain, key_norm_gain, attn_gain, residual, out_weight, ffn_gain,
     routes, route_weight, gate_weight, up_weight, down_weight) = args
    tokens, width = residual.shape
    full, hidden = gate_weight.shape[1:]
    half = tokens // 2
    block_rows, total_rows = BLOCK_ROWS * half // 8, TOTAL_ROWS * half // 8
    rest = half - total_rows
    hbm = pl.BlockSpec(memory_space=pl.ANY)
    heads = queries.shape[1] // head
    f32, bf16 = jnp.float32, jnp.bfloat16
    dma = pltpu.SemaphoreType.DMA
    vmem = pl.BlockSpec(memory_space=pltpu.VMEM)
    positions = np.arange(n * tokens)
    steps = np.float32(THETA) ** (-np.arange(0, head // 2, 2, dtype=np.float32) / np.float32(head // 2))
    angles = np.concatenate(
        [
            (positions // GRID_W).astype(np.float32)[:, None] * steps,
            (positions % GRID_W).astype(np.float32)[:, None] * steps,
        ],
        axis=1,
    ).reshape(n, tokens, head // 2).transpose(0, 2, 1)
    rows = max(8, n)
    pairs = heads // 2
    return pl.pallas_call(
        functools.partial(layer_kernel, n, head, block_rows, total_rows),
        out_shape=jax.ShapeDtypeStruct((tokens, width), bf16),
        in_specs=[hbm] * 16,
        out_specs=vmem,
        scratch_shapes=[
            pltpu.VMEM((head // 2, tokens), f32),
            pltpu.VMEM((head // 2, tokens), f32),
            pltpu.VMEM((head, tokens), bf16),
            pltpu.VMEM((head, tokens), bf16),
            pltpu.VMEM((1, head), f32),
            pltpu.VMEM((1, head), f32),
            pltpu.VMEM(queries.shape, bf16),
            pltpu.VMEM(routes.shape[::-1], jnp.int32),
            pltpu.VMEM(routes.shape[::-1], f32),
            pltpu.VMEM((1, out_weight.shape[0]), f32),
            pltpu.VMEM(out_weight.shape, bf16),
            pltpu.VMEM((tokens, width), bf16),
            pltpu.VMEM((full, hidden), bf16),
            pltpu.VMEM((full, hidden), bf16),
            pltpu.VMEM((hidden, full), bf16),
            pltpu.VMEM((4, 1, width), f32),
            pltpu.VMEM((n, 1, tokens), f32),
            pltpu.VMEM((n, tokens, 128), f32),
            dma((n,)), dma((n,)), dma((3,)), dma((4,)),
            pltpu.VMEM((n, 2, 2, 2, half, width), bf16),
            pltpu.VMEM((tokens, width), bf16),
            pltpu.VMEM((n, tokens, 128), f32),
            dma((16,)),
            pltpu.VMEM((n, 2, head, tokens), bf16),
            pltpu.VMEM((heads, tokens, 128), bf16),
            pltpu.VMEM((heads, tokens, 128), f32),
            pltpu.VMEM((heads, tokens, 128), f32),
            pltpu.VMEM((heads, tokens, 128), f32),
            pltpu.VMEM((4, pairs, tokens, 128), bf16),
            pltpu.VMEM((4, 1, tokens), f32),
            pltpu.VMEM((rows, 1, tokens), f32),
            pltpu.VMEM((rows, 1, tokens), f32),
            dma((n // 2, 2)), dma((n, 2)), dma((n // 2, 2)), dma((n,)), dma((n,)),
            dma((3, pairs)), dma((4, pairs)), dma((3,)), dma((4,)),
            pltpu.VMEM((n, 2, tokens, width), bf16),
            pltpu.VMEM((n, 2, tokens, width), bf16),
            pltpu.VMEM((n, 2, rest, width), bf16),
            pltpu.VMEM((n, 2, rest, width), bf16),
            pltpu.VMEM((n, 2, 2, half, width), bf16),
            pltpu.VMEM((n, 2, 2, half, width), bf16),
            pltpu.VMEM((4, 2, tokens, width), f32),
            pltpu.VMEM((2, total_rows, width), bf16),
            pltpu.VMEM((2, total_rows, width), bf16),
            dma((2,)), dma((2,)), dma((2, n)), dma((2, n)),
            dma((2, 3, n)), dma((2, 3, n)), dma((2, 2, n)), dma((2, 2, n)),
            dma((2, n)), dma((2, n)), dma((2, n)), dma((2, n)),
            dma((2, 3, n)), dma((2, 3, n)), dma((2,)), dma((2,)),
        ],
        compiler_params=pltpu.CompilerParams(
            collective_id=0, has_side_effects=True, vmem_limit_bytes=60 * 1024 * 1024
        ),
    )(
        np.cos(angles).astype(np.float32), np.sin(angles).astype(np.float32),
        keys.T, values.T, key_norm_gain.reshape(1, head), query_gain.reshape(1, head), queries,
        routes.T, route_weight.T, attn_gain.reshape(1, -1), ffn_gain.reshape(1, -1), out_weight, residual,
        gate_weight, up_weight, down_weight,
    )


def per_device(
    queries,
    keys,
    values,
    query_gain,
    key_norm_gain,
    attn_gain,
    residual,
    out_weight,
    ffn_gain,
    routes,
    route_weight,
    gate_weight,
    up_weight,
    down_weight,
):
    tokens = queries.shape[0]
    head_size = query_gain.shape[0]
    experts = lax.axis_size("sp")
    paired = experts >= 4 and experts & (experts - 1) == 0 and experts <= 2 * routes.shape[1]
    if paired and lax.axis_size("tp") == 4 and keys.shape[1] == head_size == 64:
        return whole_layer(
            (queries, keys, values, query_gain, key_norm_gain, attn_gain, residual, out_weight,
             ffn_gain, routes, route_weight, gate_weight, up_weight, down_weight),
            experts, head_size,
        )
    kv_local = keys.shape[1] // head_size
    q_local = queries.shape[1] // head_size
    group_width = q_local // kv_local
    first_token = lax.axis_index("sp") * tokens
    positions = first_token + jnp.arange(tokens, dtype=jnp.int32)
    cosine_lookup, sine_lookup = rotary_tables(positions, head_size, GRID_W)
    query_rotated = normalize_then_rotate(
        queries.reshape(tokens, q_local, head_size), query_gain, cosine_lookup, sine_lookup
    )
    key_rotated = normalize_then_rotate(
        keys.reshape(tokens, kv_local, head_size), key_norm_gain, cosine_lookup, sine_lookup
    )
    query_rows = query_rotated.reshape(tokens, kv_local, group_width, head_size).transpose(
        1, 0, 2, 3
    )
    query_rows = query_rows.reshape(kv_local, tokens * group_width, head_size)
    value_rows = values.reshape(tokens, kv_local, head_size)
    score_scale = head_size ** (-0.5)
    query_width = tokens * group_width
    start_state = (
        jnp.full((kv_local, query_width), -1e30, jnp.float32),
        jnp.zeros((kv_local, query_width), jnp.float32),
        jnp.zeros((kv_local, query_width, head_size), jnp.float32),
    )
    kv_width = kv_local * head_size
    packed = jnp.concatenate([key_rotated.reshape(tokens, kv_width), values], axis=1)
    gathered = lax.all_gather(packed, "sp", axis=0, tiled=True)
    piece_keys = gathered[:, :kv_width].reshape(-1, kv_local, head_size)
    piece_values = gathered[:, kv_width:].reshape(-1, kv_local, head_size)
    slot_count = piece_keys.shape[0]
    block_rows = 2048
    key_blocks = piece_keys.reshape(slot_count // block_rows, block_rows, kv_local, head_size)
    value_blocks = piece_values.reshape(slot_count // block_rows, block_rows, kv_local, head_size)

    def one_block(softmax_state, pair_block):
        running_max, running_sum, accumulated = softmax_state
        key_block, value_block = pair_block
        scores = (
            jnp.einsum("kqd,nkd->kqn", query_rows, key_block, preferred_element_type=jnp.float32)
            * score_scale
        )
        new_max = jnp.maximum(running_max, jnp.max(scores, axis=-1))
        weights = jnp.exp(scores - new_max[..., None])
        factor = jnp.exp(running_max - new_max)
        running_sum = running_sum * factor + jnp.sum(weights, axis=-1)
        accumulated = accumulated * factor[..., None] + jnp.einsum(
            "kqn,nkd->kqd",
            weights.astype(jnp.bfloat16),
            value_block,
            preferred_element_type=jnp.float32,
        )
        return ((new_max, running_sum, accumulated), None)

    final_state, unused_out = lax.scan(one_block, start_state, (key_blocks, value_blocks))
    running_max, running_sum, accumulated = final_state
    attended = (accumulated / running_sum[..., None]).reshape(
        kv_local, tokens, group_width, head_size
    )
    attended = (
        attended.transpose(1, 0, 2, 3).reshape(tokens, q_local * head_size).astype(jnp.bfloat16)
    )
    all_heads = lax.all_gather(attended, "tp", axis=1, tiled=True)
    head_f = all_heads.astype(jnp.float32)
    attn_normed = (
        head_f * lax.rsqrt(jnp.mean(head_f * head_f, axis=-1, keepdims=True) + EPS) * attn_gain
    ).astype(jnp.bfloat16)
    mid_stream = (
        residual.astype(jnp.float32)
        + jnp.dot(attn_normed, out_weight, preferred_element_type=jnp.float32)
    ).astype(jnp.bfloat16)
    mid_f = mid_stream.astype(jnp.float32)
    square_total = lax.psum(jnp.sum(mid_f * mid_f, axis=-1), "tp")
    ffn_in = (mid_f * lax.rsqrt(square_total / D + EPS)[:, None] * ffn_gain).astype(jnp.bfloat16)
    top_k = routes.shape[1]
    capacity = tokens * top_k * 3 // (2 * experts)
    route_list = routes.reshape(-1)
    onehot = (route_list[:, None] == jnp.arange(experts, dtype=jnp.int32)[None, :]).astype(
        jnp.int32
    )
    route_ranks = jnp.sum((jnp.cumsum(onehot, axis=0) - 1) * onehot, axis=1)
    slot_index = route_list * capacity + route_ranks
    slot_owner = (
        jnp.full((experts * capacity,), tokens, jnp.int32)
        .at[slot_index]
        .set(jnp.arange(tokens * top_k, dtype=jnp.int32) // top_k)
    )
    padded = jnp.concatenate([ffn_in, jnp.zeros((1, ffn_in.shape[1]), ffn_in.dtype)], axis=0)
    slot_block = lax.all_to_all(
        padded[slot_owner].reshape(experts, capacity, ffn_in.shape[1]),
        "sp",
        split_axis=0,
        concat_axis=0,
        tiled=True,
    )
    slot_count = slot_block.shape[1]
    slot_rows = slot_block.reshape(-1, slot_block.shape[2])
    column_piece = lax.all_gather(slot_rows, "tp", axis=1, tiled=True)
    gate_rows = gate_weight[0]
    up_rows = up_weight[0]
    gate_sum = jnp.dot(column_piece, gate_rows, preferred_element_type=jnp.float32)
    up_sum = jnp.dot(column_piece, up_rows, preferred_element_type=jnp.float32)
    partial_value = jnp.dot(
        clamped_unit(gate_sum, up_sum), down_weight[0], preferred_element_type=jnp.float32
    )
    summed = lax.psum_scatter(
        partial_value.astype(jnp.bfloat16), "tp", scatter_dimension=1, tiled=True
    )
    results = lax.all_to_all(
        summed.reshape(experts, slot_count, summed.shape[1]),
        "sp",
        split_axis=0,
        concat_axis=0,
        tiled=True,
    )
    picked = results.reshape(experts * capacity, -1)[slot_index].astype(jnp.float32)
    weighted = jnp.sum(
        (picked * route_weight.reshape(-1)[:, None]).reshape(tokens, top_k, -1), axis=1
    )
    return (mid_f + weighted).astype(jnp.bfloat16)


def solution(mesh):
    placed = (
        P("sp", "tp"),
        P("sp", "tp"),
        P("sp", "tp"),
        P(),
        P(),
        P(),
        P("sp", "tp"),
        P(None, "tp"),
        P("tp"),
        P("sp", None),
        P("sp", None),
        P("sp", None, "tp"),
        P("sp", None, "tp"),
        P("sp", "tp", None),
    )
    return jax.shard_map(
        per_device, mesh=mesh, in_specs=placed, out_specs=P("sp", "tp"), check_vma=False
    )
```

```python
import functools

import jax
import jax.numpy as jnp
import numpy as np
from jax import lax
from jax.experimental import pallas as pl
from jax.experimental.pallas import tpu as pltpu
from jax.sharding import PartitionSpec as P

D = 2048
GRID_W = 64


EPS = 1e-06
THETA = 10000.0
ALPHA = 1.702
LIMIT = 7.0
BLOCK_ROWS = 4
TOTAL_ROWS = 3


def rotary_tables(positions, head_size, grid_width):
    row_pos = (positions // grid_width).astype(jnp.float32)
    col_pos = (positions % grid_width).astype(jnp.float32)
    half_size = head_size // 2
    inverse = THETA ** (-jnp.arange(0, half_size, 2, dtype=jnp.float32) / half_size)
    angles = jnp.concatenate([row_pos[:, None] * inverse, col_pos[:, None] * inverse], axis=-1)
    return (jnp.cos(angles), jnp.sin(angles))


def normalize_then_rotate(head_rows, gain_vector, cosine_lookup, sine_lookup):
    values_f = head_rows.astype(jnp.float32)
    scaled = (
        values_f
        * lax.rsqrt(jnp.mean(values_f * values_f, axis=-1, keepdims=True) + EPS)
        * gain_vector
    )
    first_half, second_half = jnp.split(scaled, 2, axis=-1)
    cos_part = cosine_lookup[:, None, :]
    sin_part = sine_lookup[:, None, :]
    return jnp.concatenate(
        [
            first_half * cos_part - second_half * sin_part,
            first_half * sin_part + second_half * cos_part,
        ],
        axis=-1,
    ).astype(jnp.bfloat16)


def clamped_unit(gate_sum, up_sum):
    gate_sum = jnp.minimum(gate_sum, LIMIT)
    up_sum = jnp.clip(up_sum, -LIMIT, LIMIT)
    return ((up_sum + 1.0) * gate_sum * jax.nn.sigmoid(ALPHA * gate_sum)).astype(jnp.bfloat16)


def ring_place(device, n):
    odd = lax.rem(device, 2)
    far = device // 2
    return (1 - odd) * far + odd * (n - 1 - far)


def ring_device(place, n):
    odd = place // (n // 2)
    return 2 * ((1 - odd) * place + odd * (n - 1 - place)) + odd


def expert_phase(
    n, block_rows, total_rows, held, gate_ref, up_ref, down_ref, share_ref, inv_ref, gain_all, settle, gather_norms, mid_ref, out_ref,
    core_out, core_in, sum_out, sum_in, ring_in, ring_out, kept, last_out, last_in,
    f_send, f_recv, x_send, x_recv, g_send, g_recv, c_send, c_recv,
    cs_send, cs_recv, xs_send, xs_recv, r_send, r_recv, l_send, l_recv,
):
    f32, bf16 = jnp.float32, jnp.bfloat16
    me = lax.axis_index("sp")
    tp = lax.axis_index("tp")
    core = lax.rem(tp, 2)
    side = tp // 2
    place = ring_place(me, n)
    targets = (ring_device(lax.rem(place + 1, n), n), ring_device(lax.rem(place + n - 1, n), n))
    other_core = side * 2 + 1 - core
    other_side = (1 - side) * 2 + core
    half = held.shape[4]
    width = held.shape[5]
    rest = half - total_rows
    block_head, block_tail = pl.ds(0, block_rows), pl.ds(block_rows, half - block_rows)
    total_head, total_tail = pl.ds(0, total_rows), pl.ds(total_rows, rest)
    block_parts = ((0, block_tail), (0, block_head), (1, block_head))
    total_parts = ((0, total_head), (1, total_head), (0, total_tail))

    def owner(h, step):
        return ring_device(lax.rem(place + (n - step if h == 0 else step), n), n)

    def side_of(which):
        return side if which == 0 else 1 - side

    def first_copy(h):
        block = held.at[me, h, core, side, block_head]
        return remote(block, block, f_send.at[h], f_recv.at[h], (me, other_side))

    def first_arrival(h):
        block = held.at[me, h, core, 1 - side, block_head]
        return remote(block, block, f_send.at[h], f_recv.at[h], (me, other_side))

    def side_copy(h, step):
        block = held.at[owner(h, step), h, core, side, block_tail]
        return remote(block, block, x_send.at[h, step], x_recv.at[h, step], (me, other_side))

    def side_arrival(h, step):
        block = held.at[owner(h, step), h, core, 1 - side, block_tail]
        return remote(block, block, x_send.at[h, step], x_recv.at[h, step], (me, other_side))

    def ring_copy(h, step, i):
        which, rows = block_parts[i]
        block = held.at[owner(h, step), h, core, side_of(which), rows]
        return remote(
            block, block, g_send.at[h, i, step], g_recv.at[h, i, step + 1], (targets[h], tp)
        )

    def ring_arrival(h, step, i):
        which, rows = block_parts[i]
        block = held.at[owner(h, step), h, core, side_of(which), rows]
        return remote(block, block, g_send.at[h, i, step], g_recv.at[h, i, step], (targets[h], tp))

    def core_copy(which, h, step):
        block = held.at[owner(h, step), h, core, side_of(which)]
        return remote(
            block, block, c_send.at[which, h, step], c_recv.at[which, h, step], (me, other_core)
        )

    def core_arrival(which, h, step):
        block = held.at[owner(h, step), h, 1 - core, side_of(which)]
        return remote(
            block, block, c_send.at[which, h, step], c_recv.at[which, h, step], (me, other_core)
        )

    def core_sums(which, step):
        return remote(
            core_out.at[step, which], core_in.at[step, which],
            cs_send.at[which, step], cs_recv.at[which, step], (me, other_core),
        )

    def side_sums(h, step):
        return remote(
            sum_out.at[step, h], sum_in.at[step, h],
            xs_send.at[h, step], xs_recv.at[h, step], (me, other_side),
        )

    def total_copy(h, step, i):
        which, rows = total_parts[i]
        later = lax.rem(step + 1, n)
        return remote(
            ring_out.at[step, h, which, rows], ring_in.at[later, h, which, rows],
            r_send.at[h, i, step], r_recv.at[h, i, later], (targets[h], tp),
        )

    def total_arrival(h, step, i):
        which, rows = total_parts[i]
        return remote(
            ring_out.at[step, h, which, rows], ring_in.at[step, h, which, rows],
            r_send.at[h, i, step], r_recv.at[h, i, step], (targets[h], tp),
        )

    def last_copy(h):
        return remote(last_out.at[h], last_in.at[h], l_send.at[h], l_recv.at[h], (me, other_side))

    for h in range(2):
        first_copy(h).start()
    ring_in[1] = jnp.zeros(ring_in.shape[1:], bf16)

    def pass_part(step, i):
        for h in range(2):
            @pl.when(step > 0)
            def _():
                ring_arrival(h, step, i).wait_recv()

            if i == 2:
                @pl.when(step == 0)
                def _():
                    first_arrival(h).wait_recv()

            @pl.when(step < n - 1)
            def _():
                ring_copy(h, step, i).start()

            if i == 1:
                core_copy(0, h, step).start()

    def send_side(step):
        for h in range(2):
            side_copy(h, step).start()

    def share_sides(step):
        for h in range(2):
            side_arrival(h, step).wait_recv()
            core_copy(1, h, step).start()

    def normed_rows(block, h, t):
        inverse = inv_ref[block, h * half : (h + 1) * half]
        inverse = jnp.concatenate([inverse] * (width // 128), axis=1)
        return (held[block, h, t % 2, t // 2].astype(f32) * inverse * gain_all[t]).astype(bf16)

    def compute(step):
        now = lax.rem(step, kept.shape[0])
        for h in range(2):
            for which in range(2):
                core_arrival(which, h, step).wait_recv()
        owners = (owner(0, step), owner(1, step))
        rows = jnp.concatenate(
            [
                jnp.concatenate([normed_rows(owners[h], h, t) for t in range(4)], axis=1)
                for h in range(2)
            ],
            axis=0,
        )
        gate_sum = jnp.dot(rows, gate_ref[...], preferred_element_type=f32)
        up_sum = jnp.dot(rows, up_ref[...], preferred_element_type=f32)
        units = clamped_unit(gate_sum, up_sum)
        share = jnp.concatenate(
            [share_ref[owners[h], h * half : (h + 1) * half] for h in range(2)], axis=0
        )
        share = jnp.concatenate([share] * (width // 128), axis=1)

        def part_of(c, which):
            columns = pl.ds(pl.multiple_of((2 * side_of(which) + c) * width, width), width)
            return jnp.dot(units, down_ref[:, columns], preferred_element_type=f32) * share

        for which in (1, 0):
            core_out[step, which] = part_of(1 - core, which).astype(bf16)
            core_sums(which, step).start()
        for which in (1, 0):
            kept[now, which] = part_of(core, which)

    def total_part(step, i):
        now = lax.rem(step, kept.shape[0])
        which, rows = total_parts[i]
        for h in range(2):
            start = h * half + rows.start
            value = kept[now, which, start : start + rows.size]
            if i == 2:
                side_sums(h, step).wait_recv()
                value = value + sum_in[step, h].astype(f32)

            @pl.when(step > 1)
            def _():
                total_arrival(h, step, i).wait_recv()

            ring_out[step, h, which, rows] = (
                value + ring_in[step, h, which, rows].astype(f32)
            ).astype(bf16)
            total_copy(h, step, i).start()

    def pair_sums(step):
        now = lax.rem(step, kept.shape[0])
        for which in (1, 0):
            core_sums(which, step).wait_recv()
            value = kept[now, which] + core_in[step, which].astype(f32)
            if which == 1:
                for h in range(2):
                    sum_out[step, h] = value[h * half + total_rows : (h + 1) * half].astype(bf16)
                    side_sums(h, step).start()
            kept[now, which] = value

    order = (
        (lambda step: pass_part(step, 0), 0, 0, n - 1),
        (send_side, 0, 0, n - 1),
        (lambda step: total_part(step, 0), 5, 1, n - 1),
        (lambda step: pair_sums(lax.rem(step, n)), 3, 1, n),
        (lambda step: total_part(step, 1), 3, 1, n - 1),
        (lambda step: pass_part(step, 1), 0, 0, n - 1),
        (lambda step: compute(lax.rem(step, n)), 2, 1, n),
        (lambda step: pass_part(step, 2), 1, 0, n - 1),
        (share_sides, 1, 0, n - 1),
        (lambda step: total_part(step, 2), 4, 1, n - 1),
        (lambda step: settle(), 0, 0, 0),
        (lambda step: gather_norms(), 2, 0, 0),
    )

    def one_step(i, carry):
        for run, lag, low, high in order:
            pl.when((i >= low + lag) & (i <= high + lag))(functools.partial(run, i - lag))
        return carry

    lax.fori_loop(0, n + 5, one_step, 0)
    for h in range(2):
        rows = pl.ds(h * half, total_rows)
        total_arrival(h, 0, 1).wait_recv()
        last_out[h] = (kept[0, 1, rows] + ring_in[0, h, 1, total_head].astype(f32)).astype(bf16)
        last_copy(h).start()
    for h in range(2):
        rows = pl.ds(h * half + total_rows, rest)
        total_arrival(h, 0, 2).wait_recv()
        side_sums(h, 0).wait_recv()
        value = kept[0, 0, rows] + ring_in[0, h, 0, total_tail].astype(f32) + sum_in[0, h].astype(f32)
        out_ref[rows, :] = (mid_ref[rows, :].astype(f32) + value).astype(bf16)
    for h in range(2):
        rows = pl.ds(h * half, total_rows)
        total_arrival(h, 0, 0).wait_recv()
        last_copy(h).wait_recv()
        value = kept[0, 0, rows] + ring_in[0, h, 0, total_head].astype(f32) + last_in[h].astype(f32)
        out_ref[rows, :] = (mid_ref[rows, :].astype(f32) + value).astype(bf16)
        first_copy(h).wait_send()
        last_copy(h).wait_send()

    def finish(step, carry):
        for h in range(2):
            side_copy(h, step).wait_send()
            side_sums(h, step).wait_send()
            core_sums(h, step).wait_send()
            for which in range(2):
                core_copy(which, h, step).wait_send()
            for i in range(3):
                @pl.when(step < n - 1)
                def _():
                    ring_copy(h, step, i).wait_send()

                @pl.when(step > 0)
                def _():
                    total_copy(h, step, i).wait_send()

        return carry

    lax.fori_loop(0, n, finish, 0)


def flip(z, k, bits):
    out = 0
    for b in range(bits):
        zb = (z // (1 << b)) % 2
        kb = (k // (1 << b)) % 2
        out = out + (zb + kb - 2 * zb * kb) * (1 << b)
    return out


def remote(src, dst, send, recv, peer):
    return pltpu.make_async_remote_copy(
        src_ref=src, dst_ref=dst, send_sem=send, recv_sem=recv,
        device_id=peer, device_id_type=pl.DeviceIdType.MESH,
    )


def lanes_to_rows(row):
    return jnp.transpose(jnp.broadcast_to(row, (128, row.shape[1])))


def layer_kernel(
    n, head, block_rows, total_rows, *refs
):
    sources, out_ref, landings, refs = refs[:16], refs[16], refs[17:32], refs[32:]
    layer_body(n, head, block_rows, total_rows, sources, out_ref, landings, *refs)


def layer_body(
    n, head, block_rows, total_rows, sources, out_ref, landings, gain_all, inv_all, inv_ref,
    n_send, n_recv, gs_send, gs_recv,
    held, mid_ref, share_ref, w_sem,
    kv_all, q_all, m_s, l_s, acc, att_all, ss_all, sh_own, sh_all,
    z_send, kv_recv, y_send, sh_send, sh_recv, a_send, a_recv, s_send, s_recv,
    *expert_refs,
):
    (cos_ref, sin_ref, kt_ref, vt_ref, kg_ref, qg_ref, q_ref, rt_ref, rw_ref, ag_ref, w_ref, res_ref,
     gate_ref, up_ref, down_ref) = landings
    f32, bf16 = jnp.float32, jnp.bfloat16
    me = lax.axis_index("sp")
    tp = lax.axis_index("tp")
    core = tp % 2
    side = tp // 2
    other_core = side * 2 + 1 - core
    other_side = (1 - side) * 2 + core
    corner = (1 - side) * 2 + 1 - core
    nz = n // 2
    bits = nz.bit_length() - 1
    z = me // 2
    y = me % 2
    pair = 2 * z + 1 - y
    tokens = q_ref.shape[0]
    heads = q_ref.shape[1] // head
    quarter = head // 2

    barrier = pltpu.get_barrier_semaphore()
    for d in range(1, n):
        pl.semaphore_signal(
            barrier, inc=1, device_id=((me + d) % n, tp), device_id_type=pl.DeviceIdType.MESH
        )
    for peer in (other_core, other_side, corner):
        pl.semaphore_signal(
            barrier, inc=1, device_id=(me, peer), device_id_type=pl.DeviceIdType.MESH
        )

    sources = [src.at[me] for src in sources[:2]] + list(sources[2:13]) + [
        src.at[0] for src in sources[13:]
    ]
    landings = landings[:2] + landings[2:10] + (gain_all.at[tp],) + landings[10:]
    loads = [
        pltpu.make_async_copy(src, dst, w_sem.at[i])
        for i, (src, dst) in enumerate(zip(sources, landings))
    ]
    for load in loads:
        load.start()
    for load in loads[:5]:
        load.wait()
    cos_t = cos_ref[...]
    sin_t = sin_ref[...]
    key = kt_ref[...].astype(f32)
    gain_rows = lanes_to_rows(jnp.concatenate([kg_ref[...], kg_ref[...]], axis=1))[:head, :1]
    mean = jnp.sum(key * key, axis=0, keepdims=True) / head
    scaled = key * lax.rsqrt(mean + EPS) * gain_rows
    first, second = scaled[:quarter], scaled[quarter:]
    kv_all[me, 0, :quarter, :] = (first * cos_t - second * sin_t).astype(bf16)
    kv_all[me, 0, quarter:, :] = (first * sin_t + second * cos_t).astype(bf16)
    kv_all[me, 1] = vt_ref[...]

    for load in loads[5:11]:
        load.wait()
    cos_q = jnp.transpose(jnp.concatenate([cos_t] * 4, axis=0))
    sin_q = jnp.transpose(jnp.concatenate([-sin_t, sin_t] * 2, axis=0))
    lane = lax.broadcasted_iota(jnp.int32, (tokens, 128), 1)
    low = lane < head
    near = lane % head < quarter
    gain_q = jnp.concatenate([qg_ref[...], qg_ref[...]], axis=1)
    for j in range(heads // 2):
        x = q_ref[:, 128 * j : 128 * (j + 1)].astype(f32)
        square = x * x
        even = jnp.sum(jnp.where(low, square, 0.0), axis=1, keepdims=True)
        odd = jnp.sum(jnp.where(low, 0.0, square), axis=1, keepdims=True)
        inverse = lax.rsqrt(jnp.where(low, even, odd) / head + EPS)
        scaled = x * inverse * gain_q
        partner = jnp.where(
            near, pltpu.roll(scaled, 128 - quarter, 1), pltpu.roll(scaled, quarter, 1)
        )
        turned = (scaled * cos_q + partner * sin_q).astype(bf16).astype(f32) * (head**-0.5)
        q_all[2 * j] = jnp.where(low, turned, 0.0).astype(bf16)
        q_all[2 * j + 1] = jnp.where(low, 0.0, turned).astype(bf16)

    m_s[...] = jnp.full(m_s.shape, -1e30, f32)
    l_s[...] = jnp.zeros(l_s.shape, f32)
    acc[...] = jnp.zeros(acc.shape, f32)

    pl.semaphore_wait(barrier, n + 2)

    inner = ((z + 1) // 2) % 2

    def partner(k):
        swapped = k + (k // 2) % 2 * (1 - 2 * (k % 2))
        return flip(z, inner * ((nz - k) % nz) + (1 - inner) * swapped, bits)

    def z_copy(k, c):
        return remote(
            kv_all.at[me, c], kv_all.at[me, c], z_send.at[k, c], kv_recv.at[me, c],
            (2 * flip(z, k, bits) + y, tp),
        )

    def y_copy(k, c):
        block = 2 * partner(k) + y
        return remote(
            kv_all.at[block, c], kv_all.at[block, c], y_send.at[k, c], kv_recv.at[block, c], (pair, tp)
        )

    def arrival(block, c):
        return remote(
            kv_all.at[block, c], kv_all.at[block, c], z_send.at[0, c], kv_recv.at[block, c], (pair, tp)
        )

    for c in range(2):
        y_copy(0, c).start()
    for k in range(nz - 1, 0, -1):
        for c in range(2):
            z_copy(k, c).start()
    peers = (other_side, corner, other_core)

    def gain_copy(i, slot, peer):
        return remote(gain_all.at[slot], gain_all.at[slot], gs_send.at[i], gs_recv.at[slot], (me, peer))

    for i, peer in enumerate(peers):
        gain_copy(i, tp, peer).start()

    chosen = jnp.zeros((sh_all.shape[0], tokens), f32)
    expert = lax.broadcasted_iota(jnp.int32, chosen.shape, 0)
    for k in range(rt_ref.shape[0]):
        chosen = chosen + jnp.where(expert == rt_ref[k : k + 1, :], rw_ref[k : k + 1, :], 0.0)
    for e in range(n):
        sh_own[e] = chosen[e : e + 1, :]

    def share_copy(d):
        to = (me + d) % n
        return remote(sh_own.at[to], sh_all.at[me], sh_send.at[d], sh_recv.at[me], (to, tp))

    def share_arrival(d):
        block = (me + n - d) % n
        return remote(sh_own.at[me], sh_all.at[block], sh_send.at[d], sh_recv.at[block], (block, tp))

    for d in range(1, n):
        share_copy(d).start()
    sh_all[me] = sh_own[me]

    def attend(k, which):
        other = 2 * partner(k) + 1 - y
        mine = 2 * partner(k) + y
        keys = jnp.concatenate([kv_all[mine, 0], kv_all[other, 0]], axis=1)
        values = jnp.concatenate([kv_all[mine, 1], kv_all[other, 1]], axis=1)
        kk = jnp.concatenate([keys, keys], axis=0)
        vv = jnp.concatenate([values, values], axis=0)
        pieces = keys.shape[1] // 128
        for h in which:
            scores = jnp.dot(q_all[h], kk, preferred_element_type=f32)
            old = m_s[h]
            new = jnp.maximum(old, jnp.max(scores, axis=1, keepdims=True))
            weights = jnp.exp(scores - jnp.concatenate([new] * pieces, axis=1))
            factor = jnp.exp(old - new)
            part = weights[:, :128]
            for i in range(1, pieces):
                part = part + weights[:, 128 * i : 128 * (i + 1)]
            l_s[h] = l_s[h] * factor + part
            acc[h] = acc[h] * factor + lax.dot_general(
                weights.astype(bf16), vv, (((1,), (1,)), ((), ())), preferred_element_type=f32
            )
            m_s[h] = new

    def group_step(k, carry):
        for c in range(2):
            arrival(2 * partner(k + 1) + y, c).wait_recv()
            y_copy(k + 1, c).start()
        for c in range(2):
            arrival(2 * partner(k) + 1 - y, c).wait_recv()
        attend(k, range(heads))
        return carry

    lax.fori_loop(0, nz - 1, group_step, 0)

    def head_copy(i, j, slot, peer):
        return remote(
            att_all.at[slot, j], att_all.at[slot, j], a_send.at[i, j], a_recv.at[slot, j], (me, peer)
        )

    for c in range(2):
        arrival(2 * partner(nz - 1) + 1 - y, c).wait_recv()
    for j in range(heads // 2):
        attend(nz - 1, (2 * j, 2 * j + 1))
        even = acc[2 * j] / jnp.sum(l_s[2 * j], axis=1, keepdims=True)
        odd = acc[2 * j + 1] / jnp.sum(l_s[2 * j + 1], axis=1, keepdims=True)
        att_all[tp, j] = jnp.where(low, even, odd).astype(bf16)
        head_copy(0, j, tp, other_side).start()
        head_copy(1, j, tp, other_core).start()
    for d in range(1, n):
        share_arrival(d).wait_recv()
    for b in range(n):
        share_ref[b] = lanes_to_rows(sh_all[b])
    for j in range(heads // 2):
        head_copy(0, j, other_side, other_side).wait_recv()
        head_copy(2, j, other_side, other_core).start()
    for j in range(heads // 2):
        head_copy(1, j, other_core, other_core).wait_recv()
        head_copy(2, j, corner, other_core).wait_recv()

    loads[11].wait()
    loads[12].wait()
    every = jnp.concatenate(
        [att_all[t, j] for t in range(4) for j in range(heads // 2)], axis=1
    ).astype(f32)
    mean = jnp.mean(every * every, axis=1, keepdims=True)
    normed = (every * lax.rsqrt(mean + EPS) * ag_ref[...]).astype(bf16)
    mid = (
        res_ref[...].astype(f32) + jnp.dot(normed, w_ref[...], preferred_element_type=f32)
    ).astype(bf16)
    mid_ref[...] = mid
    mid_f = mid.astype(f32)
    square = mid_f * mid_f
    width = mid.shape[1]
    part = square[:, :128]
    for i in range(1, width // 128):
        part = part + square[:, 128 * i : 128 * (i + 1)]
    ss_all[tp] = jnp.sum(jnp.transpose(part), axis=0, keepdims=True)

    def sum_copy(i, slot, peer):
        return remote(ss_all.at[slot], ss_all.at[slot], s_send.at[i], s_recv.at[slot], (me, peer))

    for i, peer in enumerate(peers):
        sum_copy(i, tp, peer).start()
    half = tokens // 2
    for h in range(2):
        held[me, h, core, side] = mid[h * half : (h + 1) * half]

    def norm_copy(d):
        to = (me + d) % n
        return remote(inv_all.at[me], inv_all.at[me], n_send.at[d], n_recv.at[me], (to, tp))

    def norm_arrival(d):
        block = (me + n - d) % n
        return remote(inv_all.at[block], inv_all.at[block], n_send.at[d], n_recv.at[block], (block, tp))

    def settle():
        for i, peer in enumerate(peers):
            sum_copy(i, peer, peer).wait_recv()
        total = (ss_all[0] + ss_all[1]) + (ss_all[2] + ss_all[3])
        inv_all[me] = lax.rsqrt(total / (4 * width) + EPS)
        for d in range(1, n):
            norm_copy(d).start()

    def gather_norms():
        for d in range(1, n):
            norm_arrival(d).wait_recv()
        for i, peer in enumerate(peers):
            gain_copy(i, peer, peer).wait_recv()
        for b in range(n):
            inv_ref[b] = lanes_to_rows(inv_all[b])

    for load in loads[13:]:
        load.wait()
    expert_phase(
        n, block_rows, total_rows, held, gate_ref, up_ref, down_ref, share_ref,
        inv_ref, gain_all, settle, gather_norms, mid_ref, out_ref, *expert_refs
    )

    for c in range(2):
        for k in range(nz):
            y_copy(k, c).wait_send()
        for k in range(1, nz):
            z_copy(k, c).wait_send()
    for d in range(1, n):
        share_copy(d).wait_send()
    for j in range(heads // 2):
        head_copy(0, j, tp, other_side).wait_send()
        head_copy(1, j, tp, other_core).wait_send()
        head_copy(2, j, other_side, other_core).wait_send()
    for d in range(1, n):
        norm_copy(d).wait_send()
    for i, peer in enumerate(peers):
        sum_copy(i, tp, peer).wait_send()
        gain_copy(i, tp, peer).wait_send()


def whole_layer(args, n, head):
    (queries, keys, values, query_gain, key_norm_gain, attn_gain, residual, out_weight, ffn_gain,
     routes, route_weight, gate_weight, up_weight, down_weight) = args
    tokens, width = residual.shape
    full, hidden = gate_weight.shape[1:]
    half = tokens // 2
    block_rows, total_rows = BLOCK_ROWS * half // 8, TOTAL_ROWS * half // 8
    rest = half - total_rows
    hbm = pl.BlockSpec(memory_space=pl.ANY)
    heads = queries.shape[1] // head
    f32, bf16 = jnp.float32, jnp.bfloat16
    dma = pltpu.SemaphoreType.DMA
    vmem = pl.BlockSpec(memory_space=pltpu.VMEM)
    positions = np.arange(n * tokens)
    steps = np.float32(THETA) ** (-np.arange(0, head // 2, 2, dtype=np.float32) / np.float32(head // 2))
    angles = np.concatenate(
        [
            (positions // GRID_W).astype(np.float32)[:, None] * steps,
            (positions % GRID_W).astype(np.float32)[:, None] * steps,
        ],
        axis=1,
    ).reshape(n, tokens, head // 2).transpose(0, 2, 1)
    rows = max(8, n)
    pairs = heads // 2
    return pl.pallas_call(
        functools.partial(layer_kernel, n, head, block_rows, total_rows),
        out_shape=pltpu.VMEM((tokens, width), bf16),
        in_specs=[hbm] * 16,
        out_specs=vmem,
        scratch_shapes=[
            pltpu.VMEM((head // 2, tokens), f32),
            pltpu.VMEM((head // 2, tokens), f32),
            pltpu.VMEM((head, tokens), bf16),
            pltpu.VMEM((head, tokens), bf16),
            pltpu.VMEM((1, head), f32),
            pltpu.VMEM((1, head), f32),
            pltpu.VMEM(queries.shape, bf16),
            pltpu.VMEM(routes.shape[::-1], jnp.int32),
            pltpu.VMEM(routes.shape[::-1], f32),
            pltpu.VMEM((1, out_weight.shape[0]), f32),
            pltpu.VMEM(out_weight.shape, bf16),
            pltpu.VMEM((tokens, width), bf16),
            pltpu.VMEM((full, hidden), bf16),
            pltpu.VMEM((full, hidden), bf16),
            pltpu.VMEM((hidden, full), bf16),
            pltpu.VMEM((4, 1, width), f32),
            pltpu.VMEM((n, 1, tokens), f32),
            pltpu.VMEM((n, tokens, 128), f32),
            dma((n,)), dma((n,)), dma((3,)), dma((4,)),
            pltpu.VMEM((n, 2, 2, 2, half, width), bf16),
            pltpu.VMEM((tokens, width), bf16),
            pltpu.VMEM((n, tokens, 128), f32),
            dma((16,)),
            pltpu.VMEM((n, 2, head, tokens), bf16),
            pltpu.VMEM((heads, tokens, 128), bf16),
            pltpu.VMEM((heads, tokens, 128), f32),
            pltpu.VMEM((heads, tokens, 128), f32),
            pltpu.VMEM((heads, tokens, 128), f32),
            pltpu.VMEM((4, pairs, tokens, 128), bf16),
            pltpu.VMEM((4, 1, tokens), f32),
            pltpu.VMEM((rows, 1, tokens), f32),
            pltpu.VMEM((rows, 1, tokens), f32),
            dma((n // 2, 2)), dma((n, 2)), dma((n // 2, 2)), dma((n,)), dma((n,)),
            dma((3, pairs)), dma((4, pairs)), dma((3,)), dma((4,)),
            pltpu.VMEM((n, 2, tokens, width), bf16),
            pltpu.VMEM((n, 2, tokens, width), bf16),
            pltpu.VMEM((n, 2, rest, width), bf16),
            pltpu.VMEM((n, 2, rest, width), bf16),
            pltpu.VMEM((n, 2, 2, half, width), bf16),
            pltpu.VMEM((n, 2, 2, half, width), bf16),
            pltpu.VMEM((4, 2, tokens, width), f32),
            pltpu.VMEM((2, total_rows, width), bf16),
            pltpu.VMEM((2, total_rows, width), bf16),
            dma((2,)), dma((2,)), dma((2, n)), dma((2, n)),
            dma((2, 3, n)), dma((2, 3, n)), dma((2, 2, n)), dma((2, 2, n)),
            dma((2, n)), dma((2, n)), dma((2, n)), dma((2, n)),
            dma((2, 3, n)), dma((2, 3, n)), dma((2,)), dma((2,)),
        ],
        compiler_params=pltpu.CompilerParams(
            collective_id=0, has_side_effects=True, vmem_limit_bytes=60 * 1024 * 1024
        ),
    )(
        np.cos(angles).astype(np.float32), np.sin(angles).astype(np.float32),
        keys.T, values.T, key_norm_gain.reshape(1, head), query_gain.reshape(1, head), queries,
        routes.T, route_weight.T, attn_gain.reshape(1, -1), ffn_gain.reshape(1, -1), out_weight, residual,
        gate_weight, up_weight, down_weight,
    )


def per_device(
    queries,
    keys,
    values,
    query_gain,
    key_norm_gain,
    attn_gain,
    residual,
    out_weight,
    ffn_gain,
    routes,
    route_weight,
    gate_weight,
    up_weight,
    down_weight,
):
    tokens = queries.shape[0]
    head_size = query_gain.shape[0]
    experts = lax.axis_size("sp")
    paired = experts >= 4 and experts & (experts - 1) == 0 and experts <= 2 * routes.shape[1]
    if paired and lax.axis_size("tp") == 4 and keys.shape[1] == head_size == 64:
        return whole_layer(
            (queries, keys, values, query_gain, key_norm_gain, attn_gain, residual, out_weight,
             ffn_gain, routes, route_weight, gate_weight, up_weight, down_weight),
            experts, head_size,
        )
    kv_local = keys.shape[1] // head_size
    q_local = queries.shape[1] // head_size
    group_width = q_local // kv_local
    first_token = lax.axis_index("sp") * tokens
    positions = first_token + jnp.arange(tokens, dtype=jnp.int32)
    cosine_lookup, sine_lookup = rotary_tables(positions, head_size, GRID_W)
    query_rotated = normalize_then_rotate(
        queries.reshape(tokens, q_local, head_size), query_gain, cosine_lookup, sine_lookup
    )
    key_rotated = normalize_then_rotate(
        keys.reshape(tokens, kv_local, head_size), key_norm_gain, cosine_lookup, sine_lookup
    )
    query_rows = query_rotated.reshape(tokens, kv_local, group_width, head_size).transpose(
        1, 0, 2, 3
    )
    query_rows = query_rows.reshape(kv_local, tokens * group_width, head_size)
    value_rows = values.reshape(tokens, kv_local, head_size)
    score_scale = head_size ** (-0.5)
    query_width = tokens * group_width
    start_state = (
        jnp.full((kv_local, query_width), -1e30, jnp.float32),
        jnp.zeros((kv_local, query_width), jnp.float32),
        jnp.zeros((kv_local, query_width, head_size), jnp.float32),
    )
    kv_width = kv_local * head_size
    packed = jnp.concatenate([key_rotated.reshape(tokens, kv_width), values], axis=1)
    gathered = lax.all_gather(packed, "sp", axis=0, tiled=True)
    piece_keys = gathered[:, :kv_width].reshape(-1, kv_local, head_size)
    piece_values = gathered[:, kv_width:].reshape(-1, kv_local, head_size)
    slot_count = piece_keys.shape[0]
    block_rows = 2048
    key_blocks = piece_keys.reshape(slot_count // block_rows, block_rows, kv_local, head_size)
    value_blocks = piece_values.reshape(slot_count // block_rows, block_rows, kv_local, head_size)

    def one_block(softmax_state, pair_block):
        running_max, running_sum, accumulated = softmax_state
        key_block, value_block = pair_block
        scores = (
            jnp.einsum("kqd,nkd->kqn", query_rows, key_block, preferred_element_type=jnp.float32)
            * score_scale
        )
        new_max = jnp.maximum(running_max, jnp.max(scores, axis=-1))
        weights = jnp.exp(scores - new_max[..., None])
        factor = jnp.exp(running_max - new_max)
        running_sum = running_sum * factor + jnp.sum(weights, axis=-1)
        accumulated = accumulated * factor[..., None] + jnp.einsum(
            "kqn,nkd->kqd",
            weights.astype(jnp.bfloat16),
            value_block,
            preferred_element_type=jnp.float32,
        )
        return ((new_max, running_sum, accumulated), None)

    final_state, unused_out = lax.scan(one_block, start_state, (key_blocks, value_blocks))
    running_max, running_sum, accumulated = final_state
    attended = (accumulated / running_sum[..., None]).reshape(
        kv_local, tokens, group_width, head_size
    )
    attended = (
        attended.transpose(1, 0, 2, 3).reshape(tokens, q_local * head_size).astype(jnp.bfloat16)
    )
    all_heads = lax.all_gather(attended, "tp", axis=1, tiled=True)
    head_f = all_heads.astype(jnp.float32)
    attn_normed = (
        head_f * lax.rsqrt(jnp.mean(head_f * head_f, axis=-1, keepdims=True) + EPS) * attn_gain
    ).astype(jnp.bfloat16)
    mid_stream = (
        residual.astype(jnp.float32)
        + jnp.dot(attn_normed, out_weight, preferred_element_type=jnp.float32)
    ).astype(jnp.bfloat16)
    mid_f = mid_stream.astype(jnp.float32)
    square_total = lax.psum(jnp.sum(mid_f * mid_f, axis=-1), "tp")
    ffn_in = (mid_f * lax.rsqrt(square_total / D + EPS)[:, None] * ffn_gain).astype(jnp.bfloat16)
    top_k = routes.shape[1]
    capacity = tokens * top_k * 3 // (2 * experts)
    route_list = routes.reshape(-1)
    onehot = (route_list[:, None] == jnp.arange(experts, dtype=jnp.int32)[None, :]).astype(
        jnp.int32
    )
    route_ranks = jnp.sum((jnp.cumsum(onehot, axis=0) - 1) * onehot, axis=1)
    slot_index = route_list * capacity + route_ranks
    slot_owner = (
        jnp.full((experts * capacity,), tokens, jnp.int32)
        .at[slot_index]
        .set(jnp.arange(tokens * top_k, dtype=jnp.int32) // top_k)
    )
    padded = jnp.concatenate([ffn_in, jnp.zeros((1, ffn_in.shape[1]), ffn_in.dtype)], axis=0)
    slot_block = lax.all_to_all(
        padded[slot_owner].reshape(experts, capacity, ffn_in.shape[1]),
        "sp",
        split_axis=0,
        concat_axis=0,
        tiled=True,
    )
    slot_count = slot_block.shape[1]
    slot_rows = slot_block.reshape(-1, slot_block.shape[2])
    column_piece = lax.all_gather(slot_rows, "tp", axis=1, tiled=True)
    gate_rows = gate_weight[0]
    up_rows = up_weight[0]
    gate_sum = jnp.dot(column_piece, gate_rows, preferred_element_type=jnp.float32)
    up_sum = jnp.dot(column_piece, up_rows, preferred_element_type=jnp.float32)
    partial_value = jnp.dot(
        clamped_unit(gate_sum, up_sum), down_weight[0], preferred_element_type=jnp.float32
    )
    summed = lax.psum_scatter(
        partial_value.astype(jnp.bfloat16), "tp", scatter_dimension=1, tiled=True
    )
    results = lax.all_to_all(
        summed.reshape(experts, slot_count, summed.shape[1]),
        "sp",
        split_axis=0,
        concat_axis=0,
        tiled=True,
    )
    picked = results.reshape(experts * capacity, -1)[slot_index].astype(jnp.float32)
    weighted = jnp.sum(
        (picked * route_weight.reshape(-1)[:, None]).reshape(tokens, top_k, -1), axis=1
    )
    return (mid_f + weighted).astype(jnp.bfloat16)


def solution(mesh):
    placed = (
        P("sp", "tp"),
        P("sp", "tp"),
        P("sp", "tp"),
        P(),
        P(),
        P(),
        P("sp", "tp"),
        P(None, "tp"),
        P("tp"),
        P("sp", None),
        P("sp", None),
        P("sp", None, "tp"),
        P("sp", None, "tp"),
        P("sp", "tp", None),
    )
    return jax.shard_map(
        per_device, mesh=mesh, in_specs=placed, out_specs=P("sp", "tp"), check_vma=False
    )
```
